32 devices in a mesh: sp: 16 (over z, x, core), tp: 2 (over y).
Axes of the slice: x: 2, y: 2, z: 4, core: 2. Of those that a mesh axis runs over, the one named last changes fastest.
Arguments:
- skip_connection_stream: bfloat16 [12288, 2048], P('sp'), may hold values from -6 to 6
- probing_vectors: bfloat16 [12288, 512], P('sp', 'tp'), may hold values from -6 to 6
- addressing_vectors: bfloat16 [12288, 512], P('sp', 'tp'), may hold values from -6 to 6
- mapped_payloads: bfloat16 [12288, 1024], P('sp', 'tp'), may hold values from -6 to 6
- emission_switch: bfloat16 [12288, 1024], P('sp', 'tp'), may hold values from -6 to 6
- lapse_preactivation: bfloat16 [12288, 512], P('sp', 'tp')
- lapse_shift_entries: float32 [512], P('tp')
- surplus_attenuation_terms: float32 [12288], P('sp'), may hold values from -0.7 to 0
- passage_label_per_token: int32 [12288], P('sp'), may hold values from 0 to 3, never falling along the last dimension, each value on 1 to 6144 neighbouring positions
- attention_group_rescaler: float32 [128], replicated, may hold values from 0.1 to 1.9
- emission_projector: bfloat16 [1024, 2048], P('tp'), may hold values from -0.1875 to 0.1875
- perceptron_rescaler: float32 [2048], replicated, may hold values from 0.1 to 1.9
- switching_projector: bfloat16 [2048, 5632], P('sp', 'tp'), may hold values from -0.125 to 0.125
- widening_projector: bfloat16 [2048, 5632], P('sp', 'tp'), may hold values from -0.125 to 0.125
- shrinking_projector: bfloat16 [5632, 2048], P('tp', 'sp'), may hold values from -0.078125 to 0.078125
Outputs:
- layer_out: bfloat16 [12288, 2048], P(('sp', 'tp'))
The draws below stay inside these ranges and needn't reach their ends.
Inputs may be any that keep to these rules, and one draw needn't show every extreme that they name: `passage_label_per_token`: document numbers never fall along the sequence; a document holds at most 6144 positions.
All inputs are finite; a program needn't handle non-finite values.
Results may differ from the reference program's by a relative error of at most 0.014.
Values may be sent and summed in bfloat16 or wider, within the bound.
A program may use at most 128 MiB of HBM per device.

```python
import math
import jax
import jax.numpy as jnp
import numpy as np
from jax import lax

D = 2048
HEADS = 8
DK = 64
DV = 128
FF = 5632
BLOCK = 64
TOK_DEV = 768
TOKENS = 12288
DOCS = 4
DOC_MOST = 6144
N_SP = 16
N_TP = 2


def draw_lapse_preactivation(key, part):
    base_key, block_key = jax.random.split(jax.random.fold_in(key, 11))
    width = HEADS * DK
    noise = jax.random.normal(base_key, (TOKENS, width), jnp.float32)
    shift = jax.random.uniform(block_key, (TOKENS // TOK_DEV, 1, width), jnp.float32, -0.7, 0.7)
    shaped = noise.reshape(TOKENS // TOK_DEV, TOK_DEV, width) + shift
    return shaped.reshape(TOKENS, width).astype(jnp.bfloat16)


def draw_lapse_shift_entries(key, part):
    pick_key, slow_key, fast_key = jax.random.split(jax.random.fold_in(key, 23), 3)
    slow = jax.random.randint(pick_key, (HEADS,), 0, 2) > 0
    slow_vals = jnp.log(TOKENS / 16.0) + jax.random.uniform(slow_key, (HEADS, DK), jnp.float32, -1.0, 0.5)
    fast_vals = jax.random.uniform(fast_key, (HEADS, DK), jnp.float32, -0.5, 1.5)
    return jnp.where(slow[:, None], slow_vals, fast_vals).reshape(HEADS * DK).astype(jnp.float32)


def draw_surplus_attenuation_terms(key, part):
    where_key, size_key = jax.random.split(jax.random.fold_in(key, 37))
    number = max(TOKENS // TOK_DEV, 4)
    spots = jax.random.randint(where_key, (number,), 0, TOKENS)
    depth = jnp.log(jax.random.uniform(size_key, (number,), jnp.float32, 0.5, 0.8))
    return jnp.zeros((TOKENS,), jnp.float32).at[spots].min(depth)


def steps_of(stream_key, shape, pieces, low, largest):
    def one(axis_at, shards_of):
        heights = jax.random.uniform(jax.random.fold_in(jax.random.fold_in(stream_key, 6), axis_at), (shards_of,), jnp.float32, low / len(pieces), largest / len(pieces))
        return jnp.repeat(jnp.exp(heights), shape[axis_at] // shards_of).reshape((-1,) + (1,) * (len(shape) - axis_at - 1))

    factor_of = one(*pieces[0])
    for cut in pieces[1:]:
        factor_of = factor_of * one(*cut)
    return factor_of


def profile(number_of, total, most, skew):
    portions = [(1 << 20) // math.isqrt(standing ** skew) + 1 for standing in range(2, number_of + 1)]
    surplus, holding = total - most - (number_of - 1), [1] * (number_of - 1)
    while surplus > 0:
        movable = [i for i in range(number_of - 1) if holding[i] < most]
        mass, remaining = sum([portions[i] for i in movable]), surplus
        for i in movable:
            extra = min(most - holding[i], max(1, remaining * portions[i] // mass), surplus)
            holding[i] = holding[i] + extra
            surplus = surplus - extra
    return np.array([most] + holding)


def uneven(rng, number_of, total, limit, skew):
    if number_of == 2:
        one = jax.random.randint(rng, (), max(1, total - limit), min(limit, total - 1) + 1)
        return jnp.stack([one, total - one])
    lengths = jnp.asarray(profile(number_of, total, limit, skew), jnp.int32)
    twos = (number_of - 1) // 2
    giver, receiver = lengths[1:1 + 2 * twos:2], lengths[2:2 + 2 * twos:2]
    slack = jnp.minimum(giver - 1, limit - receiver)
    passed = jax.random.randint(jax.random.fold_in(rng, 1), (twos,), 0, 1 << 20) % (slack + 1)
    lengths = lengths.at[1:1 + 2 * twos:2].set(giver - passed).at[2:2 + 2 * twos:2].set(receiver + passed)
    return lengths[jax.random.permutation(jax.random.fold_in(rng, 2), number_of)]


def scatter_about(own_key, shape, scale, reach, cuts=(), kind=jnp.bfloat16):
    drawn = scale * jax.random.normal(own_key, shape, jnp.float32)
    if cuts:
        drawn = drawn * steps_of(own_key, shape, cuts, -0.22, 0.18)
    return jnp.clip(drawn, -reach, reach).astype(kind)


def setup_inputs(seed: int = 0) -> dict:
    splits = jax.random.split(jax.random.key(seed), 16)
    skip_connection_stream = scatter_about(splits[0], (TOKENS, D), 1.0, 6.0, ((0, 16),))
    probing_vectors = scatter_about(splits[1], (TOKENS, HEADS * DK), 1.0, 6.0, ((0, 16), (1, 2)))
    addressing_vectors = scatter_about(splits[2], (TOKENS, HEADS * DK), 1.0, 6.0, ((0, 16), (1, 2)))
    mapped_payloads = scatter_about(splits[3], (TOKENS, HEADS * DV), 1.0, 6.0, ((0, 16), (1, 2)))
    emission_switch = scatter_about(splits[4], (TOKENS, HEADS * DV), 1.0, 6.0, ((0, 16), (1, 2)))
    lapse_preactivation = draw_lapse_preactivation(jax.random.fold_in(splits[15], 71), 0)
    lapse_shift_entries = draw_lapse_shift_entries(jax.random.fold_in(splits[15], 71), 0)
    surplus_attenuation_terms = draw_surplus_attenuation_terms(jax.random.fold_in(splits[15], 71), 0)
    passage_label_per_token = jnp.searchsorted(jnp.cumsum(uneven(splits[8], DOCS, TOKENS, DOC_MOST, 1)), jnp.arange(TOKENS), side="right").astype(jnp.int32)
    attention_group_rescaler = jnp.clip(1.0 + 0.18 * jax.random.normal(splits[9], (DV,), jnp.float32), 0.1, 1.9)
    emission_projector = scatter_about(splits[10], (HEADS * DV, D), (HEADS * DV) ** -0.5, 0.1875, ((0, 2),))
    perceptron_rescaler = jnp.clip(1.0 + 0.18 * jax.random.normal(splits[11], (D,), jnp.float32), 0.1, 1.9)
    switching_projector = scatter_about(splits[12], (D, FF), D ** -0.5, 0.125, ((0, 16), (1, 2)))
    widening_projector = scatter_about(splits[13], (D, FF), D ** -0.5, 0.125, ((0, 16), (1, 2)))
    shrinking_projector = scatter_about(splits[14], (FF, D), FF ** -0.5, 0.078125, ((0, 2), (1, 16)))
    return {"skip_connection_stream": skip_connection_stream, "probing_vectors": probing_vectors, "addressing_vectors": addressing_vectors, "mapped_payloads": mapped_payloads, "emission_switch": emission_switch, "lapse_preactivation": lapse_preactivation, "lapse_shift_entries": lapse_shift_entries, "surplus_attenuation_terms": surplus_attenuation_terms, "passage_label_per_token": passage_label_per_token, "attention_group_rescaler": attention_group_rescaler, "emission_projector": emission_projector, "perceptron_rescaler": perceptron_rescaler, "switching_projector": switching_projector, "widening_projector": widening_projector, "shrinking_projector": shrinking_projector}


eps = 1e-06
sharpness_factor = 16.0

def head_split(array, heads):
    return array.reshape(array.shape[0], heads, -1).transpose(1, 0, 2)

def rounded(value):
    return lax.optimization_barrier(value.astype(jnp.bfloat16)).astype(jnp.float32)

def block_pass(query_head_rows, key_heads, value_heads, decay_heads, documents, recurrent_state, last_doc, offset, span):
    heads, length, _ = query_head_rows.shape
    blocks = length // span

    def to_blocks(array):
        return array.reshape(heads, blocks, span, array.shape[-1]).transpose(1, 0, 2, 3)
    lower = jnp.tril(jnp.ones((span, span), dtype=bool))

    def step(carry, inputs):
        recurrent_state, last_doc, offset = carry
        query_block, key_blk, value_block, piece_attenuation, doc_blk = inputs
        cumulative_decay = jnp.cumsum(piece_attenuation, axis=1)
        previous_valid = (doc_blk == last_doc).astype(jnp.float32)
        cross_block_output = jnp.einsum('gfl,glm->gfm', query_block * jnp.exp(cumulative_decay), recurrent_state, precision=lax.Precision.HIGHEST) * previous_valid[None, :, None]
        spread = cumulative_decay[:, :, None, :] - cumulative_decay[:, None, :, :]
        same = (doc_blk[:, None] == doc_blk[None, :]) & lower
        weights = jnp.exp(jnp.where(same[None, :, :, None], spread, -jnp.inf))
        scores = jnp.einsum('hik,hjk,hijk->hij', query_block, key_blk, weights, precision=lax.Precision.HIGHEST)
        result = cross_block_output + jnp.einsum('hij,hjv->hiv', scores, value_block, precision=lax.Precision.HIGHEST)
        final_memory_summary = cumulative_decay[:, -1, :]
        last_valid = (doc_blk[-1] == last_doc).astype(jnp.float32)
        tail_ok = (doc_blk == doc_blk[-1]).astype(jnp.float32)
        decayed_keys = key_blk * jnp.exp(final_memory_summary[:, None, :] - cumulative_decay) * tail_ok[None, :, None]
        recurrent_state = recurrent_state * jnp.exp(final_memory_summary)[:, :, None] * last_valid + jnp.einsum('wrz,wrs->wzs', decayed_keys, value_block, precision=lax.Precision.HIGHEST)
        return ((recurrent_state, doc_blk[-1], offset + final_memory_summary), (result, cumulative_decay + offset[:, None, :]))
    carry, outputs = lax.scan(step, (recurrent_state, last_doc, offset), (to_blocks(query_head_rows), to_blocks(key_heads), to_blocks(value_heads), to_blocks(decay_heads), documents.reshape(blocks, span)))
    result, running_state = outputs
    result = result.transpose(1, 0, 2, 3).reshape(heads, length, -1)
    running_state = running_state.transpose(1, 0, 2, 3).reshape(heads, length, -1)
    return (carry[0], carry[2], result, running_state)

def reference(skip_connection_stream, probing_vectors, addressing_vectors, mapped_payloads, emission_switch, lapse_preactivation, lapse_shift_entries, surplus_attenuation_terms, passage_label_per_token, attention_group_rescaler, emission_projector, perceptron_rescaler, switching_projector, widening_projector, shrinking_projector):
    keeping_exponent = jax.nn.log_sigmoid(lapse_preactivation.astype(jnp.float32) + lapse_shift_entries[None, :]) / sharpness_factor + surplus_attenuation_terms[:, None]
    query_head_rows = head_split(probing_vectors.astype(jnp.float32) * DK ** (-0.5), HEADS)
    key_heads = head_split(addressing_vectors.astype(jnp.float32), HEADS)
    value_heads = head_split(mapped_payloads.astype(jnp.float32), HEADS)
    decay_heads = head_split(keeping_exponent, HEADS)
    zero_state = jnp.zeros((HEADS, DK, DV), jnp.float32)
    _, _, attn, _ = block_pass(query_head_rows, key_heads, value_heads, decay_heads, passage_label_per_token, zero_state, jnp.array(-1, jnp.int32), jnp.zeros((HEADS, DK), jnp.float32), BLOCK)
    normed_attn = attn * lax.rsqrt(lax.optimization_barrier(jnp.mean(attn * attn, axis=-1, keepdims=True)) + eps) * attention_group_rescaler
    flat = normed_attn.transpose(1, 0, 2).reshape(attn.shape[1], HEADS * DV)
    gated = (flat * jax.nn.silu(emission_switch.astype(jnp.float32))).astype(jnp.bfloat16)
    head_cols = HEADS * DV // N_TP
    ff_cols = FF // N_TP

    def rows_fn(index):
        start = (index * TOK_DEV).astype(jnp.int32)
        gated_rows = lax.dynamic_slice_in_dim(gated, start, TOK_DEV, 0)
        resid_rows = lax.dynamic_slice_in_dim(skip_connection_stream, start, TOK_DEV, 0)
        mixed = jnp.zeros((TOK_DEV, D), jnp.float32)
        for group in range(N_TP):
            mixed = mixed + rounded(jnp.dot(gated_rows[:, group * head_cols:(group + 1) * head_cols], emission_projector[group * head_cols:(group + 1) * head_cols], preferred_element_type=jnp.float32))
        first_resid = (resid_rows.astype(jnp.float32) + mixed).astype(jnp.bfloat16)
        wide = first_resid.astype(jnp.float32)
        normed = (wide * lax.rsqrt(lax.optimization_barrier(jnp.mean(wide * wide, axis=-1, keepdims=True)) + eps) * perceptron_rescaler).astype(jnp.bfloat16)
        gate = jnp.dot(normed, switching_projector, preferred_element_type=jnp.float32)
        upper = jnp.dot(normed, widening_projector, preferred_element_type=jnp.float32)
        hidden = (jax.nn.silu(gate) * upper).astype(jnp.bfloat16)
        ffn_out = jnp.zeros((TOK_DEV, D), jnp.float32)
        for group in range(N_TP):
            ffn_out = ffn_out + rounded(jnp.dot(hidden[:, group * ff_cols:(group + 1) * ff_cols], shrinking_projector[group * ff_cols:(group + 1) * ff_cols], preferred_element_type=jnp.float32))
        return (wide + 0.5 * ffn_out).astype(jnp.bfloat16)
    blocks_out = lax.map(rows_fn, jnp.arange(N_SP, dtype=jnp.int32))
    return blocks_out.reshape(N_SP * TOK_DEV, D)
```

```python
import functools

import jax
import jax.numpy as jnp
from jax import lax
from jax.experimental import pallas as pl
from jax.experimental.pallas import tpu as pltpu
from jax.sharding import PartitionSpec as P

DK = 64
DV = 128
BLOCK = 64
LIMIT = 80.0

eps = 1e-06
sharpness_factor = 16.0
HIGHEST = lax.Precision.HIGHEST
F32 = jnp.float32
BF16 = jnp.bfloat16


def dot0(a, b, precision=None):
    return lax.dot_general(
        a, b, (((0,), (0,)), ((), ())), precision=precision, preferred_element_type=F32
    )


def dot1(a, b, precision=None):
    return lax.dot_general(
        a, b, (((1,), (0,)), ((), ())), precision=precision, preferred_element_type=F32
    )


def local_pass(
    q_ref, k_ref, v_ref, lapse_ref, shift_ref, surplus_ref, doc_col_ref, doc_row_ref,
    out_ref, qrun_ref, state_ref, total_ref,
):
    length, width = q_ref.shape
    heads = width // DK
    span = BLOCK
    middle = span // 2
    rows = lax.broadcasted_iota(jnp.int32, (span, span), 0)
    cols = lax.broadcasted_iota(jnp.int32, (span, span), 1)
    lower = rows >= cols
    tril = lower.astype(F32)
    ones = jnp.ones((span, DV), F32)
    lane_head = lax.broadcasted_iota(jnp.int32, (span, width), 1) // DK
    head_mask = [(lane_head == h).astype(F32) for h in range(heads)]

    def per_head(a):
        return jnp.concatenate([(a * m).astype(BF16) for m in head_mask], axis=0)

    state = None
    offset = jnp.zeros((1, width), F32)
    for b in range(length // span):
        at = pl.ds(b * span, span)
        pre = lapse_ref[at, :].astype(F32) + shift_ref[...]
        ld = (jnp.minimum(pre, 0.0) - jnp.log1p(jnp.exp(-jnp.abs(pre)))) * (
            1.0 / sharpness_factor
        ) + surplus_ref[at, :]
        cum = dot1(tril, ld, HIGHEST)
        q = q_ref[at, :].astype(F32) * DK ** (-0.5)
        k = k_ref[at, :].astype(F32)
        v = v_ref[at, :]
        doc_col = doc_col_ref[at, :]
        doc_row = doc_row_ref[b : b + 1, :]
        tot = cum[span - 1 : span, :]
        centre = cum[middle : middle + 1, :]
        decayed = jnp.exp(cum)
        qd = q * decayed
        qrun_ref[at, :] = (qd * jnp.exp(offset)).astype(BF16)
        qs = q * jnp.exp(jnp.minimum(cum - centre, LIMIT))
        ks = (k * jnp.exp(jnp.minimum(centre - cum, LIMIT))).astype(BF16)
        scores = lax.dot_general(
            per_head(qs), ks, (((1,), (1,)), ((), ())), preferred_element_type=F32
        )
        same = (doc_col == doc_row) & lower
        if b > 0:
            last = doc_col_ref[b * span - 1 : b * span, :]
            valid = (doc_col == last).astype(F32)
            cross = dot1(per_head(qd), state.astype(BF16))
        for h in range(heads):
            piece = slice(h * span, (h + 1) * span)
            lanes = slice(h * DV, (h + 1) * DV)
            masked = jnp.where(same, scores[piece], 0.0).astype(BF16)
            res = dot1(masked, v[:, lanes])
            if b > 0:
                res = res + cross[piece] * valid
            out_ref[at, lanes] = res
        tail_doc = doc_col[span - 1 : span, :]
        tail_ok = (doc_col == tail_doc).astype(F32)
        kd = (k * jnp.exp(tot - cum) * tail_ok).astype(BF16)
        update = dot0(kd, v)
        update = jnp.concatenate(
            [update[h * DK : (h + 1) * DK, h * DV : (h + 1) * DV] for h in range(heads)], axis=0
        )
        if b > 0:
            keep = (tail_doc == last).astype(F32)
            state = state * (jnp.exp(dot0(ld, ones, HIGHEST)) * keep) + update
        else:
            state = update
        offset = offset + tot
    state_ref[...] = state
    total_ref[...] = offset


def finish_pass(out_ref, qrun_ref, entering_ref, reaches_ref, switch_ref, gain_ref, gated_ref):
    length, width = qrun_ref.shape
    heads = width // DK
    rows = 256 if length % 256 == 0 else length
    lane_head = lax.broadcasted_iota(jnp.int32, (rows, width), 1) // DK
    for r in range(length // rows):
        at = pl.ds(r * rows, rows)
        q = qrun_ref[at, :]
        reaches = reaches_ref[at, :]
        for h in range(heads):
            lanes = slice(h * DV, (h + 1) * DV)
            qh = jnp.where(lane_head == h, q, jnp.zeros_like(q))
            attn = out_ref[at, lanes] + dot1(qh, entering_ref[...]) * reaches
            normed = (
                attn
                * lax.rsqrt(jnp.mean(attn * attn, axis=-1, keepdims=True) + eps)
                * gain_ref[...]
            )
            s = switch_ref[at, lanes].astype(F32)
            gated_ref[at, lanes] = (normed * (s / (1.0 + jnp.exp(-s)))).astype(BF16)


def rms_rows(rows, gain):
    wide = rows.astype(F32)
    return (wide * lax.rsqrt(jnp.mean(wide * wide, axis=-1, keepdims=True) + eps) * gain).astype(
        BF16
    )


def ring_orders(n_sp):
    chips = n_sp // 2
    return list(range(0, chips, 2)) + list(range(1, chips, 2))[::-1]


def ring_pairs(n_sp, step):
    ring = ring_orders(n_sp)
    count = len(ring)
    return [
        (2 * ring[i] + core, 2 * ring[(i + step) % count] + core)
        for i in range(count)
        for core in (0, 1)
    ]


def swap_cores(a, n_sp):
    return lax.ppermute(a, "sp", [(i, i ^ 1) for i in range(n_sp)])


def ring_start(own, n_sp):
    return (
        lax.ppermute(own, "sp", ring_pairs(n_sp, 1)),
        lax.ppermute(own, "sp", ring_pairs(n_sp, -1)),
    )


def ring_rest(first, n_sp, axis):
    behind, ahead = [first[0]], [first[1]]
    count = n_sp // 2
    for _ in range((count - 1) // 2 - 1):
        behind.append(lax.ppermute(behind[-1], "sp", ring_pairs(n_sp, 1)))
        ahead.append(lax.ppermute(ahead[-1], "sp", ring_pairs(n_sp, -1)))
    size = first[0].shape[axis] // 2
    low = lax.slice_in_dim(behind[-1], 0, size, axis=axis)
    high = lax.slice_in_dim(ahead[-1], size, 2 * size, axis=axis)
    low = lax.ppermute(low, "sp", ring_pairs(n_sp, 1))
    high = lax.ppermute(high, "sp", ring_pairs(n_sp, -1))
    return behind, ahead, (low, high)


def vmem(n):
    return [pl.BlockSpec(memory_space=pltpu.VMEM)] * n


def per_device(
    skip_connection_stream,
    probing_vectors,
    addressing_vectors,
    mapped_payloads,
    emission_switch,
    lapse_preactivation,
    lapse_shift_entries,
    surplus_attenuation_terms,
    passage_label_per_token,
    attention_group_rescaler,
    emission_projector,
    perceptron_rescaler,
    switching_projector,
    widening_projector,
    shrinking_projector,
):
    rows_here, width = probing_vectors.shape
    heads = width // DK
    n_sp, n_tp = lax.axis_size("sp"), lax.axis_size("tp")
    place, group = lax.axis_index("sp"), lax.axis_index("tp")
    docs = passage_label_per_token

    def to_later(a, step):
        return lax.ppermute(a, "tp", [(i, (i + step) % n_tp) for i in range(n_tp)])

    both_w = jnp.concatenate([switching_projector, widening_projector], axis=1)
    both_first = ring_start(both_w, n_sp)
    down_first = ring_start(shrinking_projector, n_sp)
    projectors = [emission_projector] + [to_later(emission_projector, s) for s in range(1, n_tp)]

    local_out, qrun, state, total = pl.pallas_call(
        local_pass,
        out_shape=(
            jax.ShapeDtypeStruct((rows_here, heads * DV), F32),
            jax.ShapeDtypeStruct((rows_here, width), BF16),
            jax.ShapeDtypeStruct((width, DV), F32),
            jax.ShapeDtypeStruct((1, width), F32),
        ),
        in_specs=vmem(8),
        out_specs=tuple(vmem(4)),
        cost_estimate=pl.CostEstimate(
            flops=40_000_000_000, bytes_accessed=6_000_000, transcendentals=0
        ),
        name="local_pass",
    )(
        probing_vectors,
        addressing_vectors,
        mapped_payloads,
        lapse_preactivation,
        lapse_shift_entries[None, :],
        surplus_attenuation_terms[:, None],
        docs[:, None],
        docs.reshape(-1, BLOCK),
    )

    unbroken = (docs[0] == docs[-1]).astype(F32)
    ends = jnp.stack([docs[0], docs[-1]]).astype(BF16)
    small = jnp.concatenate([(jnp.exp(total[0]) * unbroken).astype(BF16), ends])
    tail_rows = 16 * pl.cdiv(small.size, 16 * DV)
    small = jnp.pad(small, (0, tail_rows * DV - small.size)).reshape(tail_rows, DV)
    packed = jnp.concatenate([state.astype(BF16), small], axis=0)
    half = (width + tail_rows) // 2
    first_half = lax.all_gather(packed[:half], "sp")
    packed, first_half = lax.optimization_barrier((packed, first_half))
    second_half = lax.all_gather(packed[half:], "sp")
    second_half, both_first = lax.optimization_barrier((second_half, both_first))
    packed = jnp.concatenate([first_half, second_half], axis=1)
    behind, ahead, opposite = ring_rest(both_first, n_sp, 1)
    down_first, opposite = lax.optimization_barrier((down_first, opposite))
    down_behind, down_ahead, down_opposite = ring_rest(down_first, n_sp, 0)

    ring = jnp.asarray(ring_orders(n_sp), jnp.int32)
    count = n_sp // 2
    spot = jnp.argmax(ring == place // 2)
    core = place % 2

    def chip_at(steps_behind):
        return ring[(spot - steps_behind + count) % count]

    chips = [chip_at(0)]
    chips += [chip_at(d + 1) for d in range(len(behind))]
    chips += [chip_at(-d - 1) for d in range(len(ahead))]
    chips += [chip_at(count // 2)]
    owners = [2 * c + core for c in chips] + [2 * c + 1 - core for c in chips]
    lows, highs = opposite
    here = [both_w] + behind + ahead + [jnp.concatenate([lows, highs], axis=1)]
    there = [swap_cores(a, n_sp) for a in [both_w] + behind + ahead]
    there += [jnp.concatenate([swap_cores(lows, n_sp), swap_cores(highs, n_sp)], axis=1)]
    hidden_width = switching_projector.shape[1]
    gate_w = jnp.concatenate([a[:, :hidden_width] for a in here + there], axis=0)
    up_w = jnp.concatenate([a[:, hidden_width:] for a in here + there], axis=0)
    down_here = [shrinking_projector] + down_behind + down_ahead
    down_there = [swap_cores(a, n_sp) for a in down_here]
    states = packed[:, :width]
    smalls = packed[:, width:].reshape(n_sp, -1).astype(F32)
    decays, first_doc, last_doc = smalls[:, :width], smalls[:, width], smalls[:, width + 1]
    before = jnp.concatenate([jnp.full((1,), -1.0, F32), last_doc[:-1]])
    decays = decays * (before == first_doc).astype(F32)[:, None]
    entering = jnp.zeros((width, DV), F32)
    for j in range(n_sp):
        entering = jnp.where(
            j < place, entering * decays[j][:, None] + states[j].astype(F32), entering
        )
    reaches = (docs.astype(F32) == before[place]).astype(F32)

    gated = pl.pallas_call(
        finish_pass,
        out_shape=jax.ShapeDtypeStruct((rows_here, heads * DV), BF16),
        in_specs=vmem(6),
        out_specs=vmem(1)[0],
        cost_estimate=pl.CostEstimate(
            flops=5_000_000_000, bytes_accessed=5_000_000, transcendentals=0
        ),
        name="finish_pass",
    )(
        local_out,
        qrun,
        entering.astype(BF16),
        reaches[:, None],
        emission_switch,
        attention_group_rescaler[None, :],
    )

    gateds = [gated] + [to_later(gated, s) for s in range(1, n_tp)]
    mixed = jnp.zeros((), F32)
    for rows, weight in zip(gateds, projectors):
        part = jnp.dot(rows, weight, preferred_element_type=F32).astype(BF16)
        mixed = mixed + part.astype(F32)
    first_all = (skip_connection_stream.astype(F32) + mixed).astype(BF16)
    normed = rms_rows(first_all, perceptron_rescaler)
    block = switching_projector.shape[0]

    def columns(a, owner):
        return lax.dynamic_slice_in_dim(a, owner * block, block, 1)

    ringed = jnp.concatenate([columns(normed, owner) for owner in owners], axis=1)
    gate = jnp.dot(ringed, gate_w, preferred_element_type=F32)
    upper = jnp.dot(ringed, up_w, preferred_element_type=F32)
    hidden = (jax.nn.silu(gate) * upper).astype(BF16)

    share = rows_here // n_tp

    def share_of(a, owner):
        return lax.dynamic_slice_in_dim(a, owner * share, share, 0)

    def reduced(weight):
        def down(owner):
            return jnp.dot(share_of(hidden, owner), weight, preferred_element_type=F32).astype(BF16)

        arrived = [to_later(down((group + s) % n_tp), s) for s in range(1, n_tp)]
        total = down(group).astype(F32)
        for part in arrived:
            total = total + part.astype(F32)
        return total

    late_here = jnp.concatenate(down_opposite, axis=0)
    late_there = jnp.concatenate([swap_cores(a, n_sp) for a in down_opposite], axis=0)
    near = (len(down_here) + 1) // 2
    order = [0] + [i + 1 + j * len(down_behind) for i in range(len(down_behind)) for j in (0, 1)]
    groups = [order[:near], order[near:], [len(down_here)]]
    down_here, down_there = down_here + [late_here], down_there + [late_there]
    first_own = share_of(first_all, group)
    out = first_own
    for members in groups:
        weight = jnp.concatenate(
            [down_here[i] for i in members] + [down_there[i] for i in members], axis=1
        )
        whose = [owners[i] for i in members] + [owners[len(chips) + i] for i in members]
        total = reduced(weight)
        for i, owner in enumerate(whose):
            start = (0, owner * block)
            piece = total[:, i * block : (i + 1) * block]
            base = lax.dynamic_slice(first_own, start, (share, block)).astype(F32)
            out = lax.dynamic_update_slice(out, (base + 0.5 * piece).astype(BF16), start)
    return out


MESH = pl.DeviceIdType.MESH
SPAN = BLOCK
TILE = 256
DOC_MOST = 6144


def local_copy(src, dst, sem):
    return pltpu.make_async_copy(src, dst, sem)


def column_of(row):
    first = lax.broadcasted_iota(jnp.int32, (8, row.shape[1]), 0) == 0
    return dot0(jnp.where(first, row, 0.0), jnp.ones((8, DV), F32), HIGHEST)


def ring_chip(spot, n_chip):
    return jnp.where(spot < n_chip // 2, 2 * spot, 2 * (n_chip - 1 - spot) + 1)


def ring_spot(chip, n_chip):
    return jnp.where(chip % 2 == 0, chip // 2, n_chip - 1 - chip // 2)


def fused_kernel(
    plan,
    skip_hbm, q_hbm, k_hbm, v_hbm, switch_hbm, lapse_hbm, proj_hbm, gate_hbm, up_hbm, down_hbm,
    shift_ref, docs_ref, surplus_ref, head_gain_ref, gain_ref,
    out_hbm,
    gate_all, up_all, down_all, proj_all, gated_all, first, normed, hidden,
    q_ref, k_ref, v_ref, switch_ref, lapse_ref, local_out, qrun, state, total,
    st_own, sm_own, st_sib, sm_sib, st_cmp, sm_cmp, st_in, sm_in,
    send_buf, recv_buf, out_v,
    load_sem, own_sem, ici_send, ici_recv, d2d_send, d2d_recv,
    y_send, y_recv, st_send, st_recv, red_send, red_recv, out_sem,
):
    n_chip, window, split, k_half = plan
    rows, width = q_ref.shape
    heads = width // DK
    group_w = heads * DV
    model = normed.shape[1]
    inner = hidden.shape[1]
    block = gate_hbm.shape[0]
    half = rows // 2
    pair = 2 * block

    place = lax.axis_index("sp")
    group = lax.axis_index("tp")
    core = lax.rem(place, 2)
    chip = place // 2
    reach = n_chip // 2
    spot = ring_spot(chip, n_chip)
    steps = [0] + [d for i in range(1, reach) for d in (i, -i)] + [reach]
    near = [ring_chip(lax.rem(spot + d + n_chip, n_chip), n_chip) for d in steps]
    sibling = {"sp": chip * 2 + 1 - core}
    across = {"tp": 1 - group}

    def same_core(c):
        return {"sp": c * 2 + core}

    ahead, behind = same_core(near[1]), same_core(near[2])

    def slot_of(d):
        return steps.index(d if -reach < d else d + n_chip)

    barrier = pltpu.get_barrier_semaphore()
    for j in range(1, n_chip):
        pl.semaphore_signal(
            barrier, inc=1, device_id=same_core(lax.rem(chip + j, n_chip)), device_id_type=MESH
        )
    pl.semaphore_signal(barrier, inc=1, device_id=sibling, device_id_type=MESH)
    pl.semaphore_signal(barrier, inc=1, device_id=across, device_id_type=MESH)
    pl.semaphore_wait(barrier, n_chip + 1)

    sent = []

    def remote(src, dst, send, recv, dev):
        return pltpu.make_async_remote_copy(
            src_ref=src, dst_ref=dst, send_sem=send, recv_sem=recv, device_id=dev,
            device_id_type=MESH,
        )

    def start(copy):
        copy.start()
        sent.append(copy)

    cols = [(0, split), (split, inner - split)]
    unit_rows = [block] * 4 + [k_half, inner - k_half]

    def own_view(m, r0, nr):
        if m < 4:
            c0, nc = cols[m // 2]
            return (gate_hbm, up_hbm)[m % 2].at[pl.ds(r0, nr), pl.ds(c0, nc)]
        return down_hbm.at[pl.ds((m - 4) * k_half + r0, nr), :]

    def view(m, slot, there, owner_core, r0, nr):
        if m < 4:
            c0, nc = cols[m // 2]
            row = pl.multiple_of((near[slot] * 2 + owner_core) * block + r0, 16)
            return (gate_all, up_all)[m % 2].at[pl.ds(row, nr), pl.ds(c0, nc)]
        lane = slot_of(steps[slot] - there) * pair + owner_core * block
        lanes = pl.ds(pl.multiple_of(lane, block), block)
        return down_all.at[pl.ds((m - 4) * k_half + r0, nr), lanes]

    def piece(m, i, forward):
        nr = unit_rows[m]
        if i < reach - 1:
            return 0, nr
        return (0, nr // 2) if forward else (nr // 2, nr - nr // 2)

    def hop(m, i, forward):
        r0, nr = piece(m, i, forward)
        sign = 1 if forward else -1
        slot = slot_of(-sign * i)
        src = own_view(m, r0, nr) if i == 0 else view(m, slot, 0, core, r0, nr)
        e = 2 * i + (0 if forward else 1)
        start(remote(
            src, view(m, slot, sign, core, r0, nr), ici_send.at[m, e], ici_recv.at[m, e],
            ahead if forward else behind,
        ))

    def landed(m, i, forward):
        r0, nr = piece(m, i, forward)
        sign = 1 if forward else -1
        at = view(m, slot_of(-sign * (i + 1)), 0, core, r0, nr)
        e = 2 * i + (0 if forward else 1)
        remote(at, at, ici_send.at[m, e], ici_recv.at[m, e], ahead).wait_recv()

    def hand(m, slot):
        nr = unit_rows[m]
        at = view(m, slot, 0, core, 0, nr)
        src = own_view(m, 0, nr) if slot == 0 else at
        start(remote(src, at, d2d_send.at[m, slot], d2d_recv.at[m, slot], sibling))

    def handed(m, slot):
        at = view(m, slot, 0, 1 - core, 0, unit_rows[m])
        remote(at, at, d2d_send.at[m, slot], d2d_recv.at[m, slot], sibling).wait_recv()

    def send_own(m):
        hop(m, 0, True)
        hop(m, 0, False)

    def relay(units, i):
        for m in units:
            landed(m, i, True)
            landed(m, i, False)
            if i + 1 < reach:
                hop(m, i + 1, True)
                hop(m, i + 1, False)
        for m in units:
            if i + 1 < reach:
                hand(m, slot_of(i + 1))
                hand(m, slot_of(-i - 1))
            else:
                hand(m, slot_of(reach))

    send_own(0)
    loads = [
        local_copy(q_hbm, q_ref, load_sem.at[0]),
        local_copy(k_hbm, k_ref, load_sem.at[1]),
        local_copy(v_hbm, v_ref, load_sem.at[2]),
        local_copy(lapse_hbm, lapse_ref, load_sem.at[3]),
        local_copy(switch_hbm, switch_ref, load_sem.at[4]),
        local_copy(skip_hbm, first, load_sem.at[5]),
        local_copy(proj_hbm, proj_all.at[group], load_sem.at[6]),
    ]
    for copy in loads:
        copy.start()
    p_half = proj_hbm.shape[0] // 2
    p_at = pl.ds(pl.multiple_of(core * p_half, p_half), p_half)
    p_to = remote(
        proj_hbm.at[p_at, :], proj_all.at[group, p_at, :], y_send.at[0], y_recv.at[0], across
    )
    start(p_to)
    hand(0, 0)
    keeps = []
    for m in range(6):
        keep = local_copy(
            own_view(m, 0, unit_rows[m]), view(m, 0, 0, core, 0, unit_rows[m]), own_sem.at[m]
        )
        keep.start()
        keeps.append(keep)
    for copy in loads[:4]:
        copy.wait()

    middle = SPAN // 2
    r_i = lax.broadcasted_iota(jnp.int32, (SPAN, SPAN), 0)
    c_i = lax.broadcasted_iota(jnp.int32, (SPAN, SPAN), 1)
    lane_head = lax.broadcasted_iota(jnp.int32, (SPAN, width), 1) // DK
    head_mask = [(lane_head == h).astype(F32) for h in range(heads)]

    def per_head(a):
        return jnp.concatenate([(a * m).astype(BF16) for m in head_mask], axis=0)

    def to_column(row):
        return jnp.sum(jnp.where(r_i == c_i, row, 0.0), axis=1, keepdims=True)

    state[...] = jnp.zeros_like(state)
    total[...] = jnp.zeros_like(total)
    n_block = rows // SPAN

    def attend(b, last):
        lower = r_i >= c_i
        at = pl.ds(pl.multiple_of(b * SPAN, SPAN), SPAN)
        doc_row = docs_ref[pl.ds(b, 1), :]
        doc_col = to_column(doc_row)
        sur_col = to_column(surplus_ref[pl.ds(b, 1), :])
        pre = lapse_ref[at, :].astype(F32) + shift_ref[...]
        ld = (jnp.minimum(pre, 0.0) - jnp.log1p(jnp.exp(-jnp.abs(pre)))) * (
            1.0 / sharpness_factor
        ) + sur_col
        cum = dot1(lower.astype(F32), ld, HIGHEST)
        qb = q_ref[at, :].astype(F32) * DK ** (-0.5)
        kb = k_ref[at, :].astype(F32)
        vb = v_ref[at, :]
        tot = cum[SPAN - 1 : SPAN, :]
        centre = cum[middle : middle + 1, :]
        qd = qb * jnp.exp(cum)
        offset = total[0:1, :]
        qrun[at, :] = (qd * jnp.exp(offset)).astype(BF16)
        qs = qb * jnp.exp(jnp.minimum(cum - centre, LIMIT))
        ks = (kb * jnp.exp(jnp.minimum(centre - cum, LIMIT))).astype(BF16)
        scores = lax.dot_general(
            per_head(qs), ks, (((1,), (1,)), ((), ())), preferred_element_type=F32
        )
        same = (doc_col == doc_row) & lower
        valid = (doc_col == last).astype(F32)
        cross = dot1(per_head(qd), state[...].astype(BF16))
        for h in range(heads):
            piece = slice(h * SPAN, (h + 1) * SPAN)
            lanes = slice(h * DV, (h + 1) * DV)
            masked = jnp.where(same, scores[piece], 0.0).astype(BF16)
            local_out[at, lanes] = dot1(masked, vb[:, lanes]) + cross[piece] * valid
        tail_doc = doc_row[:, SPAN - 1 : SPAN]
        tail_ok = (doc_col == tail_doc).astype(F32)
        kd = (kb * jnp.exp(tot - cum) * tail_ok).astype(BF16)
        update = dot0(kd, vb)
        update = jnp.concatenate(
            [update[h * DK : (h + 1) * DK, h * DV : (h + 1) * DV] for h in range(heads)], axis=0
        )
        keep = (tail_doc == last).astype(F32)
        state[...] = state[...] * (column_of(jnp.exp(tot)) * keep) + update
        total[...] = total[...] + tot
        return tail_doc

    last_own = lax.fori_loop(0, n_block, attend, jnp.full((1, 1), -1.0, F32))

    first_own = docs_ref[0:1, 0:1]
    row8 = lax.broadcasted_iota(jnp.int32, (8, width), 0)

    def small(decay, first_doc, last_doc):
        return jnp.where(row8 == 0, decay, jnp.where(row8 == 1, first_doc, last_doc))

    unbroken = (first_own == last_own).astype(F32)
    st_own[...] = state[...].astype(BF16)
    sm_own[...] = small(jnp.exp(total[0:1, :]) * unbroken, first_own, last_own)

    swap = [
        remote(st_own, st_sib, st_send.at[0], st_recv.at[0], sibling),
        remote(sm_own, sm_sib, st_send.at[1], st_recv.at[1], sibling),
    ]
    for copy in swap:
        start(copy)
    for copy in swap:
        copy.wait_recv()
    low = core == 0
    mine_s, mine_m = st_own[...].astype(F32), sm_own[...]
    sib_s, sib_m = st_sib[...].astype(F32), sm_sib[...]
    lo_s, hi_s = jnp.where(low, mine_s, sib_s), jnp.where(low, sib_s, mine_s)
    lo_m, hi_m = jnp.where(low, mine_m, sib_m), jnp.where(low, sib_m, mine_m)
    joined = (lo_m[2:3, 0:1] == hi_m[1:2, 0:1]).astype(F32)
    hi_decay = hi_m[0:1, :] * joined
    st_cmp[...] = (lo_s * column_of(hi_decay) + hi_s).astype(BF16)
    sm_cmp[...] = small(lo_m[0:1, :] * hi_decay, lo_m[1:2, 0:1], hi_m[2:3, 0:1])

    def composite(j):
        dev = same_core(lax.rem(chip + j, n_chip))
        return [
            remote(st_cmp, st_in.at[j - 1], st_send.at[2 * j], st_recv.at[2 * j], dev),
            remote(sm_cmp, sm_in.at[j - 1], st_send.at[2 * j + 1], st_recv.at[2 * j + 1], dev),
        ]

    for j in range(1, window + 1):

        @pl.when(chip + j < n_chip)
        def _():
            for copy in composite(j):
                copy.start()

    for m in range(1, 4):
        send_own(m)
        hand(m, 0)
    hand(4, 0)
    hand(5, 0)

    for j in range(1, window + 1):

        @pl.when(chip >= j)
        def _():
            for copy in composite(j):
                copy.wait_recv()

    entering = jnp.zeros((width, DV), F32)
    before = jnp.full((1, 1), -1.0, F32)
    for j in range(window, 0, -1):
        valid = chip >= j
        met = jnp.where(valid, sm_in[j - 1], 0.0)
        if j < window:
            linked = (before == met[1:2, 0:1]).astype(F32)
            entering = entering * column_of(met[0:1, :] * linked)
        entering = jnp.where(valid, entering + st_in[j - 1].astype(F32), 0.0)
        before = jnp.where(valid, met[2:3, 0:1], -1.0)
    linked = (before == sib_m[1:2, 0:1]).astype(F32)
    through = entering * column_of(sib_m[0:1, :] * linked) + sib_s
    st_own_f = jnp.where(low, entering, through)
    before = jnp.where(low, before, sib_m[2:3, 0:1])
    state[...] = st_own_f

    loads[4].wait()

    def finish(b, carry):
        at = pl.ds(pl.multiple_of(b * SPAN, SPAN), SPAN)
        reach = (to_column(docs_ref[pl.ds(b, 1), :]) == before).astype(F32)
        qr = qrun[at, :]
        stacked = jnp.concatenate(
            [jnp.where(lane_head == h, qr, jnp.zeros_like(qr)) for h in range(heads)], axis=0
        )
        cross = dot1(stacked, state[...].astype(BF16))
        for h in range(heads):
            lanes = slice(h * DV, (h + 1) * DV)
            attn = local_out[at, lanes] + cross[h * SPAN : (h + 1) * SPAN] * reach
            scaled = (
                attn
                * lax.rsqrt(jnp.mean(attn * attn, axis=-1, keepdims=True) + eps)
                * head_gain_ref[...]
            )
            s = switch_ref[at, lanes].astype(F32)
            gated_all[group, at, lanes] = (scaled * (s / (1.0 + jnp.exp(-s)))).astype(BF16)
        return carry

    lax.fori_loop(0, n_block, finish, 0)
    g_to = remote(
        gated_all.at[group], gated_all.at[group], y_send.at[1], y_recv.at[1], across
    )
    start(g_to)

    relay((0, 1), 0)
    p_back = remote(
        proj_all.at[1 - group, p_at, :], proj_all.at[1 - group, p_at, :],
        y_send.at[0], y_recv.at[0], across,
    )
    p_back.wait_recv()
    start(
        remote(
            proj_all.at[1 - group, p_at, :], proj_all.at[1 - group, p_at, :],
            y_send.at[2], y_recv.at[2], sibling,
        )
    )
    relay((2, 3), 0)
    for copy in loads[5:]:
        copy.wait()
    p_rest = pl.ds(pl.multiple_of((1 - core) * p_half, p_half), p_half)
    remote(
        proj_all.at[1 - group, p_rest, :], proj_all.at[1 - group, p_rest, :],
        y_send.at[2], y_recv.at[2], sibling,
    ).wait_recv()
    remote(
        gated_all.at[1 - group], gated_all.at[1 - group], y_send.at[1], y_recv.at[1], across
    ).wait_recv()
    mix_rows = 256 if rows % 256 == 0 else rows
    mix_cols = 512 if model % 512 == 0 else model

    def mix(r, carry):
        at = pl.ds(pl.multiple_of(r * mix_rows, mix_rows), mix_rows)
        squares = jnp.zeros((mix_rows, 1), F32)
        for c in range(model // mix_cols):
            lanes = slice(c * mix_cols, (c + 1) * mix_cols)
            mixed = jnp.zeros((mix_rows, mix_cols), F32)
            for g in range(2):
                part = jnp.dot(
                    gated_all[g, at, :], proj_all[g, :, lanes], preferred_element_type=F32
                )
                mixed = mixed + part.astype(BF16).astype(F32)
            new = (first[at, lanes].astype(F32) + mixed).astype(BF16)
            first[at, lanes] = new
            wide = new.astype(F32)
            squares = squares + jnp.sum(wide * wide, axis=-1, keepdims=True)
        scale = lax.rsqrt(squares * (1.0 / model) + eps)
        for c in range(model // mix_cols):
            lanes = slice(c * mix_cols, (c + 1) * mix_cols)
            normed[at, lanes] = (
                first[at, lanes].astype(F32) * scale * gain_ref[:, lanes]
            ).astype(BF16)
        return carry

    lax.fori_loop(0, rows // mix_rows, mix, 0)

    for i in range(1, reach - 1):
        relay((0, 1), i)
        relay((2, 3), i)
    for m in (4, 5):
        send_own(m)
    relay((0, 1), reach - 1)
    for m in (0, 1):
        keeps[m].wait()
        for slot in range(n_chip):
            handed(m, slot)
    def expand(t, carry):
        lanes = pl.ds(pl.multiple_of(t * TILE, TILE), TILE)
        g = jnp.dot(normed[...], gate_all[:, lanes], preferred_element_type=F32)
        u = jnp.dot(normed[...], up_all[:, lanes], preferred_element_type=F32)
        hidden[:, lanes] = (g / (1.0 + jnp.exp(-g)) * u).astype(BF16)
        return carry

    lax.fori_loop(0, split // TILE, expand, 0)

    relay((2, 3), reach - 1)
    relay((4,), 0)
    for m in (2, 3):
        keeps[m].wait()
        for slot in range(n_chip):
            handed(m, slot)
    lax.fori_loop(split // TILE, inner // TILE, expand, 0)

    own_rows = pl.ds(pl.multiple_of(group * half, half), half)

    def reduce_copy(lo, hi):
        lanes = pl.ds(lo * pair, (hi - lo) * pair)
        return remote(
            send_buf.at[:, lanes], recv_buf.at[:, lanes], red_send.at[lo], red_recv.at[lo], across
        )

    def share(part, lo, hi):
        lanes = pl.ds(lo * pair, (hi - lo) * pair)
        a, b = part[:half], part[half:]
        send_buf[:, lanes] = jnp.where(group == 0, b, a).astype(BF16)
        out_v[:, lanes] = jnp.where(group == 0, a, b).astype(BF16)
        start(reduce_copy(lo, hi))

    def shrink(lo, hi):
        lanes = pl.ds(lo * pair, (hi - lo) * pair)
        share(jnp.dot(hidden[...], down_all[:, lanes], preferred_element_type=F32), lo, hi)

    outs = []

    def settle(lo, hi):
        reduce_copy(lo, hi).wait_recv()
        for slot in range(lo, hi):
            at = pl.ds(slot * pair, pair)
            lanes = pl.ds(pl.multiple_of(near[slot] * pair, pair), pair)
            ffn = out_v[:, at].astype(F32) + recv_buf[:, at].astype(F32)
            out_v[:, at] = (first[own_rows, lanes].astype(F32) + 0.5 * ffn).astype(BF16)
            copy = local_copy(out_v.at[:, at], out_hbm.at[:, lanes], out_sem.at[slot])
            copy.start()
            outs.append(copy)

    def handed_down(slots, units=(4, 5)):
        for m in units:
            for slot in slots:
                handed(m, slot)

    relay((5,), 0)
    for m in (4, 5):
        keeps[m].wait()
    handed_down((0,))
    shrink(0, 1)
    handed_down((1, 2))
    shrink(1, 3)
    for i in range(1, reach - 1):
        relay((4,), i)
        relay((5,), i)
        handed_down((2 * i + 1, 2 * i + 2))
        shrink(2 * i + 1, 2 * i + 3)
        if i == 1:
            settle(0, 1)
        else:
            settle(2 * i - 3, 2 * i - 1)
    relay((4,), reach - 1)
    handed_down((n_chip - 1,), (4,))
    lanes = pl.ds((n_chip - 1) * pair, pair)
    part = jnp.dot(
        hidden[:, :k_half], down_all[:k_half, lanes], preferred_element_type=F32
    )
    settle(n_chip - 5, n_chip - 3)
    relay((5,), reach - 1)
    handed_down((n_chip - 1,), (5,))
    part = part + jnp.dot(
        hidden[:, k_half:], down_all[k_half:, lanes], preferred_element_type=F32
    )
    share(part, n_chip - 1, n_chip)
    settle(n_chip - 3, n_chip - 1)
    settle(n_chip - 1, n_chip)
    for copy in outs:
        copy.wait()
    for copy in sent:
        copy.wait_send()
    for j in range(1, window + 1):

        @pl.when(chip + j < n_chip)
        def _():
            for copy in composite(j):
                copy.wait_send()


def fused_per_device(
    skip_connection_stream,
    probing_vectors,
    addressing_vectors,
    mapped_payloads,
    emission_switch,
    lapse_preactivation,
    lapse_shift_entries,
    surplus_attenuation_terms,
    passage_label_per_token,
    attention_group_rescaler,
    emission_projector,
    perceptron_rescaler,
    switching_projector,
    widening_projector,
    shrinking_projector,
):
    rows, width = probing_vectors.shape
    group_w = mapped_payloads.shape[1]
    model = skip_connection_stream.shape[1]
    block, inner = switching_projector.shape
    n_sp, n_tp = lax.axis_size("sp"), lax.axis_size("tp")
    n_chip = n_sp // 2
    window = min(pl.cdiv(DOC_MOST, 2 * rows), n_chip - 1)
    tiles = inner // TILE
    split = TILE * pl.cdiv(tiles * 3, 5)
    k_half = 16 * (inner // 32)
    half = rows // 2
    pair = 2 * block
    docs = passage_label_per_token.astype(F32).reshape(-1, SPAN)
    surplus = surplus_attenuation_terms.reshape(-1, SPAN)
    DMA = pltpu.SemaphoreType.DMA
    hbm = pl.BlockSpec(memory_space=pl.ANY)
    plan = (n_chip, window, split, k_half)
    return pl.pallas_call(
        functools.partial(fused_kernel, plan),
        out_shape=jax.ShapeDtypeStruct((half, model), BF16),
        in_specs=[hbm] * 10 + vmem(5),
        out_specs=hbm,
        scratch_shapes=[
            pltpu.VMEM((model, inner), BF16),
            pltpu.VMEM((model, inner), BF16),
            pltpu.VMEM((inner, model), BF16),
            pltpu.VMEM((n_tp, group_w, model), BF16),
            pltpu.VMEM((n_tp, rows, group_w), BF16),
            pltpu.VMEM((rows, model), BF16),
            pltpu.VMEM((rows, model), BF16),
            pltpu.VMEM((rows, inner), BF16),
            pltpu.VMEM((rows, width), BF16),
            pltpu.VMEM((rows, width), BF16),
            pltpu.VMEM((rows, group_w), BF16),
            pltpu.VMEM((rows, group_w), BF16),
            pltpu.VMEM((rows, width), BF16),
            pltpu.VMEM((rows, group_w), F32),
            pltpu.VMEM((rows, width), BF16),
            pltpu.VMEM((width, DV), F32),
            pltpu.VMEM((8, width), F32),
            pltpu.VMEM((width, DV), BF16),
            pltpu.VMEM((8, width), F32),
            pltpu.VMEM((width, DV), BF16),
            pltpu.VMEM((8, width), F32),
            pltpu.VMEM((width, DV), BF16),
            pltpu.VMEM((8, width), F32),
            pltpu.VMEM((window, width, DV), BF16),
            pltpu.VMEM((window, 8, width), F32),
            pltpu.VMEM((half, model), BF16),
            pltpu.VMEM((half, model), BF16),
            pltpu.VMEM((half, model), BF16),
            DMA((7,)),
            DMA((6,)),
            DMA((6, n_chip)),
            DMA((6, n_chip)),
            DMA((6, n_chip)),
            DMA((6, n_chip)),

            DMA((3,)),
            DMA((3,)),
            DMA((2 * window + 2,)),
            DMA((2 * window + 2,)),
            DMA((n_chip,)),
            DMA((n_chip,)),
            DMA((n_chip,)),
        ],
        compiler_params=pltpu.CompilerParams(
            collective_id=0, has_side_effects=True, vmem_limit_bytes=67_043_328
        ),
        cost_estimate=pl.CostEstimate(
            flops=30_000_000_000, bytes_accessed=20_000_000, transcendentals=0
        ),
        name="fused_layer",
    )(
        skip_connection_stream,
        probing_vectors,
        addressing_vectors,
        mapped_payloads,
        emission_switch,
        lapse_preactivation,
        emission_projector,
        switching_projector,
        widening_projector,
        shrinking_projector,
        lapse_shift_entries[None, :],
        docs,
        surplus,
        attention_group_rescaler[None, :],
        perceptron_rescaler[None, :],
    )


def fits_fused(mesh, arrays):
    n_sp, n_tp = mesh.shape["sp"], mesh.shape["tp"]
    gate = arrays[12]
    block, inner = gate.shape[0] // n_sp, gate.shape[1] // n_tp
    even = n_sp % 8 == 0 and n_tp == 2
    return even and block % 128 == 0 and inner % TILE == 0 and 6 * gate.size // n_tp < 2**25 * 3 // 2


def solution(mesh):
    placed = (
        P("sp", None),
        P("sp", "tp"),
        P("sp", "tp"),
        P("sp", "tp"),
        P("sp", "tp"),
        P("sp", "tp"),
        P("tp"),
        P("sp"),
        P("sp"),
        P(),
        P("tp", None),
        P(),
        P("sp", "tp"),
        P("sp", "tp"),
        P("tp", "sp"),
    )

    def layer(*arrays):
        body = fused_per_device if fits_fused(mesh, arrays) else per_device
        return jax.shard_map(
            body, mesh=mesh, in_specs=placed, out_specs=P(("sp", "tp"), None), check_vma=False
        )(*arrays)

    return layer
```

```python
import functools

import jax
import jax.numpy as jnp
from jax import lax
from jax.experimental import pallas as pl
from jax.experimental.pallas import tpu as pltpu
from jax.sharding import PartitionSpec as P

DK = 64
DV = 128
BLOCK = 64
LIMIT = 80.0

eps = 1e-06
sharpness_factor = 16.0
HIGHEST = lax.Precision.HIGHEST
F32 = jnp.float32
BF16 = jnp.bfloat16


def dot0(a, b, precision=None):
    return lax.dot_general(
        a, b, (((0,), (0,)), ((), ())), precision=precision, preferred_element_type=F32
    )


def dot1(a, b, precision=None):
    return lax.dot_general(
        a, b, (((1,), (0,)), ((), ())), precision=precision, preferred_element_type=F32
    )


def local_pass(
    q_ref, k_ref, v_ref, lapse_ref, shift_ref, surplus_ref, doc_col_ref, doc_row_ref,
    out_ref, qrun_ref, state_ref, total_ref,
):
    length, width = q_ref.shape
    heads = width // DK
    span = BLOCK
    middle = span // 2
    rows = lax.broadcasted_iota(jnp.int32, (span, span), 0)
    cols = lax.broadcasted_iota(jnp.int32, (span, span), 1)
    lower = rows >= cols
    tril = lower.astype(F32)
    ones = jnp.ones((span, DV), F32)
    lane_head = lax.broadcasted_iota(jnp.int32, (span, width), 1) // DK
    head_mask = [(lane_head == h).astype(F32) for h in range(heads)]

    def per_head(a):
        return jnp.concatenate([(a * m).astype(BF16) for m in head_mask], axis=0)

    state = None
    offset = jnp.zeros((1, width), F32)
    for b in range(length // span):
        at = pl.ds(b * span, span)
        pre = lapse_ref[at, :].astype(F32) + shift_ref[...]
        ld = (jnp.minimum(pre, 0.0) - jnp.log1p(jnp.exp(-jnp.abs(pre)))) * (
            1.0 / sharpness_factor
        ) + surplus_ref[at, :]
        cum = dot1(tril, ld, HIGHEST)
        q = q_ref[at, :].astype(F32) * DK ** (-0.5)
        k = k_ref[at, :].astype(F32)
        v = v_ref[at, :]
        doc_col = doc_col_ref[at, :]
        doc_row = doc_row_ref[b : b + 1, :]
        tot = cum[span - 1 : span, :]
        centre = cum[middle : middle + 1, :]
        decayed = jnp.exp(cum)
        qd = q * decayed
        qrun_ref[at, :] = (qd * jnp.exp(offset)).astype(BF16)
        qs = q * jnp.exp(jnp.minimum(cum - centre, LIMIT))
        ks = (k * jnp.exp(jnp.minimum(centre - cum, LIMIT))).astype(BF16)
        scores = lax.dot_general(
            per_head(qs), ks, (((1,), (1,)), ((), ())), preferred_element_type=F32
        )
        same = (doc_col == doc_row) & lower
        if b > 0:
            last = doc_col_ref[b * span - 1 : b * span, :]
            valid = (doc_col == last).astype(F32)
            cross = dot1(per_head(qd), state.astype(BF16))
        for h in range(heads):
            piece = slice(h * span, (h + 1) * span)
            lanes = slice(h * DV, (h + 1) * DV)
            masked = jnp.where(same, scores[piece], 0.0).astype(BF16)
            res = dot1(masked, v[:, lanes])
            if b > 0:
                res = res + cross[piece] * valid
            out_ref[at, lanes] = res
        tail_doc = doc_col[span - 1 : span, :]
        tail_ok = (doc_col == tail_doc).astype(F32)
        kd = (k * jnp.exp(tot - cum) * tail_ok).astype(BF16)
        update = dot0(kd, v)
        update = jnp.concatenate(
            [update[h * DK : (h + 1) * DK, h * DV : (h + 1) * DV] for h in range(heads)], axis=0
        )
        if b > 0:
            keep = (tail_doc == last).astype(F32)
            state = state * (jnp.exp(dot0(ld, ones, HIGHEST)) * keep) + update
        else:
            state = update
        offset = offset + tot
    state_ref[...] = state
    total_ref[...] = offset


def finish_pass(out_ref, qrun_ref, entering_ref, reaches_ref, switch_ref, gain_ref, gated_ref):
    length, width = qrun_ref.shape
    heads = width // DK
    rows = 256 if length % 256 == 0 else length
    lane_head = lax.broadcasted_iota(jnp.int32, (rows, width), 1) // DK
    for r in range(length // rows):
        at = pl.ds(r * rows, rows)
        q = qrun_ref[at, :]
        reaches = reaches_ref[at, :]
        for h in range(heads):
            lanes = slice(h * DV, (h + 1) * DV)
            qh = jnp.where(lane_head == h, q, jnp.zeros_like(q))
            attn = out_ref[at, lanes] + dot1(qh, entering_ref[...]) * reaches
            normed = (
                attn
                * lax.rsqrt(jnp.mean(attn * attn, axis=-1, keepdims=True) + eps)
                * gain_ref[...]
            )
            s = switch_ref[at, lanes].astype(F32)
            gated_ref[at, lanes] = (normed * (s / (1.0 + jnp.exp(-s)))).astype(BF16)


def rms_rows(rows, gain):
    wide = rows.astype(F32)
    return (wide * lax.rsqrt(jnp.mean(wide * wide, axis=-1, keepdims=True) + eps) * gain).astype(
        BF16
    )


def ring_orders(n_sp):
    chips = n_sp // 2
    return list(range(0, chips, 2)) + list(range(1, chips, 2))[::-1]


def ring_pairs(n_sp, step):
    ring = ring_orders(n_sp)
    count = len(ring)
    return [
        (2 * ring[i] + core, 2 * ring[(i + step) % count] + core)
        for i in range(count)
        for core in (0, 1)
    ]


def swap_cores(a, n_sp):
    return lax.ppermute(a, "sp", [(i, i ^ 1) for i in range(n_sp)])


def ring_start(own, n_sp):
    return (
        lax.ppermute(own, "sp", ring_pairs(n_sp, 1)),
        lax.ppermute(own, "sp", ring_pairs(n_sp, -1)),
    )


def ring_rest(first, n_sp, axis):
    behind, ahead = [first[0]], [first[1]]
    count = n_sp // 2
    for _ in range((count - 1) // 2 - 1):
        behind.append(lax.ppermute(behind[-1], "sp", ring_pairs(n_sp, 1)))
        ahead.append(lax.ppermute(ahead[-1], "sp", ring_pairs(n_sp, -1)))
    size = first[0].shape[axis] // 2
    low = lax.slice_in_dim(behind[-1], 0, size, axis=axis)
    high = lax.slice_in_dim(ahead[-1], size, 2 * size, axis=axis)
    low = lax.ppermute(low, "sp", ring_pairs(n_sp, 1))
    high = lax.ppermute(high, "sp", ring_pairs(n_sp, -1))
    return behind, ahead, (low, high)


def vmem(n):
    return [pl.BlockSpec(memory_space=pltpu.VMEM)] * n


def per_device(
    skip_connection_stream,
    probing_vectors,
    addressing_vectors,
    mapped_payloads,
    emission_switch,
    lapse_preactivation,
    lapse_shift_entries,
    surplus_attenuation_terms,
    passage_label_per_token,
    attention_group_rescaler,
    emission_projector,
    perceptron_rescaler,
    switching_projector,
    widening_projector,
    shrinking_projector,
):
    rows_here, width = probing_vectors.shape
    heads = width // DK
    n_sp, n_tp = lax.axis_size("sp"), lax.axis_size("tp")
    place, group = lax.axis_index("sp"), lax.axis_index("tp")
    docs = passage_label_per_token

    def to_later(a, step):
        return lax.ppermute(a, "tp", [(i, (i + step) % n_tp) for i in range(n_tp)])

    both_w = jnp.concatenate([switching_projector, widening_projector], axis=1)
    both_first = ring_start(both_w, n_sp)
    down_first = ring_start(shrinking_projector, n_sp)
    projectors = [emission_projector] + [to_later(emission_projector, s) for s in range(1, n_tp)]

    local_out, qrun, state, total = pl.pallas_call(
        local_pass,
        out_shape=(
            jax.ShapeDtypeStruct((rows_here, heads * DV), F32),
            jax.ShapeDtypeStruct((rows_here, width), BF16),
            jax.ShapeDtypeStruct((width, DV), F32),
            jax.ShapeDtypeStruct((1, width), F32),
        ),
        in_specs=vmem(8),
        out_specs=tuple(vmem(4)),
        cost_estimate=pl.CostEstimate(
            flops=40_000_000_000, bytes_accessed=6_000_000, transcendentals=0
        ),
        name="local_pass",
    )(
        probing_vectors,
        addressing_vectors,
        mapped_payloads,
        lapse_preactivation,
        lapse_shift_entries[None, :],
        surplus_attenuation_terms[:, None],
        docs[:, None],
        docs.reshape(-1, BLOCK),
    )

    unbroken = (docs[0] == docs[-1]).astype(F32)
    ends = jnp.stack([docs[0], docs[-1]]).astype(BF16)
    small = jnp.concatenate([(jnp.exp(total[0]) * unbroken).astype(BF16), ends])
    tail_rows = 16 * pl.cdiv(small.size, 16 * DV)
    small = jnp.pad(small, (0, tail_rows * DV - small.size)).reshape(tail_rows, DV)
    packed = jnp.concatenate([state.astype(BF16), small], axis=0)
    half = (width + tail_rows) // 2
    first_half = lax.all_gather(packed[:half], "sp")
    packed, first_half = lax.optimization_barrier((packed, first_half))
    second_half = lax.all_gather(packed[half:], "sp")
    second_half, both_first = lax.optimization_barrier((second_half, both_first))
    packed = jnp.concatenate([first_half, second_half], axis=1)
    behind, ahead, opposite = ring_rest(both_first, n_sp, 1)
    down_first, opposite = lax.optimization_barrier((down_first, opposite))
    down_behind, down_ahead, down_opposite = ring_rest(down_first, n_sp, 0)

    ring = jnp.asarray(ring_orders(n_sp), jnp.int32)
    count = n_sp // 2
    spot = jnp.argmax(ring == place // 2)
    core = place % 2

    def chip_at(steps_behind):
        return ring[(spot - steps_behind + count) % count]

    chips = [chip_at(0)]
    chips += [chip_at(d + 1) for d in range(len(behind))]
    chips += [chip_at(-d - 1) for d in range(len(ahead))]
    chips += [chip_at(count // 2)]
    owners = [2 * c + core for c in chips] + [2 * c + 1 - core for c in chips]
    lows, highs = opposite
    here = [both_w] + behind + ahead + [jnp.concatenate([lows, highs], axis=1)]
    there = [swap_cores(a, n_sp) for a in [both_w] + behind + ahead]
    there += [jnp.concatenate([swap_cores(lows, n_sp), swap_cores(highs, n_sp)], axis=1)]
    hidden_width = switching_projector.shape[1]
    gate_w = jnp.concatenate([a[:, :hidden_width] for a in here + there], axis=0)
    up_w = jnp.concatenate([a[:, hidden_width:] for a in here + there], axis=0)
    down_here = [shrinking_projector] + down_behind + down_ahead
    down_there = [swap_cores(a, n_sp) for a in down_here]
    states = packed[:, :width]
    smalls = packed[:, width:].reshape(n_sp, -1).astype(F32)
    decays, first_doc, last_doc = smalls[:, :width], smalls[:, width], smalls[:, width + 1]
    before = jnp.concatenate([jnp.full((1,), -1.0, F32), last_doc[:-1]])
    decays = decays * (before == first_doc).astype(F32)[:, None]
    entering = jnp.zeros((width, DV), F32)
    for j in range(n_sp):
        entering = jnp.where(
            j < place, entering * decays[j][:, None] + states[j].astype(F32), entering
        )
    reaches = (docs.astype(F32) == before[place]).astype(F32)

    gated = pl.pallas_call(
        finish_pass,
        out_shape=jax.ShapeDtypeStruct((rows_here, heads * DV), BF16),
        in_specs=vmem(6),
        out_specs=vmem(1)[0],
        cost_estimate=pl.CostEstimate(
            flops=5_000_000_000, bytes_accessed=5_000_000, transcendentals=0
        ),
        name="finish_pass",
    )(
        local_out,
        qrun,
        entering.astype(BF16),
        reaches[:, None],
        emission_switch,
        attention_group_rescaler[None, :],
    )

    gateds = [gated] + [to_later(gated, s) for s in range(1, n_tp)]
    mixed = jnp.zeros((), F32)
    for rows, weight in zip(gateds, projectors):
        part = jnp.dot(rows, weight, preferred_element_type=F32).astype(BF16)
        mixed = mixed + part.astype(F32)
    first_all = (skip_connection_stream.astype(F32) + mixed).astype(BF16)
    normed = rms_rows(first_all, perceptron_rescaler)
    block = switching_projector.shape[0]

    def columns(a, owner):
        return lax.dynamic_slice_in_dim(a, owner * block, block, 1)

    ringed = jnp.concatenate([columns(normed, owner) for owner in owners], axis=1)
    gate = jnp.dot(ringed, gate_w, preferred_element_type=F32)
    upper = jnp.dot(ringed, up_w, preferred_element_type=F32)
    hidden = (jax.nn.silu(gate) * upper).astype(BF16)

    share = rows_here // n_tp

    def share_of(a, owner):
        return lax.dynamic_slice_in_dim(a, owner * share, share, 0)

    def reduced(weight):
        def down(owner):
            return jnp.dot(share_of(hidden, owner), weight, preferred_element_type=F32).astype(BF16)

        arrived = [to_later(down((group + s) % n_tp), s) for s in range(1, n_tp)]
        total = down(group).astype(F32)
        for part in arrived:
            total = total + part.astype(F32)
        return total

    late_here = jnp.concatenate(down_opposite, axis=0)
    late_there = jnp.concatenate([swap_cores(a, n_sp) for a in down_opposite], axis=0)
    near = (len(down_here) + 1) // 2
    order = [0] + [i + 1 + j * len(down_behind) for i in range(len(down_behind)) for j in (0, 1)]
    groups = [order[:near], order[near:], [len(down_here)]]
    down_here, down_there = down_here + [late_here], down_there + [late_there]
    first_own = share_of(first_all, group)
    out = first_own
    for members in groups:
        weight = jnp.concatenate(
            [down_here[i] for i in members] + [down_there[i] for i in members], axis=1
        )
        whose = [owners[i] for i in members] + [owners[len(chips) + i] for i in members]
        total = reduced(weight)
        for i, owner in enumerate(whose):
            start = (0, owner * block)
            piece = total[:, i * block : (i + 1) * block]
            base = lax.dynamic_slice(first_own, start, (share, block)).astype(F32)
            out = lax.dynamic_update_slice(out, (base + 0.5 * piece).astype(BF16), start)
    return out


MESH = pl.DeviceIdType.MESH
SPAN = BLOCK
TILE = 256
DOC_MOST = 6144


def local_copy(src, dst, sem):
    return pltpu.make_async_copy(src, dst, sem)


def column_of(row):
    first = lax.broadcasted_iota(jnp.int32, (8, row.shape[1]), 0) == 0
    return dot0(jnp.where(first, row, 0.0), jnp.ones((8, DV), F32), HIGHEST)


def ring_chip(spot, n_chip):
    return jnp.where(spot < n_chip // 2, 2 * spot, 2 * (n_chip - 1 - spot) + 1)


def ring_spot(chip, n_chip):
    return jnp.where(chip % 2 == 0, chip // 2, n_chip - 1 - chip // 2)


def fused_kernel(
    plan,
    skip_hbm, q_hbm, k_hbm, v_hbm, switch_hbm, lapse_hbm, proj_hbm, gate_hbm, up_hbm, down_hbm,
    shift_hbm, docs_hbm, surplus_hbm, head_gain_hbm, gain_hbm,
    out_ref,
    shift_ref, docs_in, surplus_in, head_gain_ref, gain_ref, docs_ref, surplus_ref,
    gate_all, up_all, down_all, proj_all, gated_all, first, normed, hidden,
    q_ref, k_ref, v_ref, switch_ref, lapse_ref, local_out, qrun, state, total,
    st_own, sm_own, st_sib, sm_sib, st_cmp, sm_cmp, st_in, sm_in,
    recv_buf,
    load_sem, ici_send, ici_recv, d2d_send, d2d_recv,
    y_send, y_recv, st_send, st_recv, red_send, red_recv,
):
    n_chip, window, split = plan
    rows, width = q_ref.shape
    heads = width // DK
    group_w = heads * DV
    model = normed.shape[1]
    inner = hidden.shape[1]
    block = gate_hbm.shape[0]
    half = rows // 2

    place = lax.axis_index("sp")
    group = lax.axis_index("tp")
    core = lax.rem(place, 2)
    chip = place // 2
    reach = n_chip // 2
    spot = ring_spot(chip, n_chip)
    steps = [0] + [d for i in range(1, reach) for d in (i, -i)] + [reach]
    near = [ring_chip(lax.rem(spot + d + n_chip, n_chip), n_chip) for d in steps]
    sibling = {"sp": chip * 2 + 1 - core}
    across = {"tp": 1 - group}

    def same_core(c):
        return {"sp": c * 2 + core}

    ahead, behind = same_core(near[1]), same_core(near[2])

    def slot_of(d):
        return steps.index(d if -reach < d else d + n_chip)

    barrier = pltpu.get_barrier_semaphore()
    for j in range(1, n_chip):
        pl.semaphore_signal(
            barrier, inc=1, device_id=same_core(lax.rem(chip + j, n_chip)), device_id_type=MESH
        )
    pl.semaphore_signal(barrier, inc=1, device_id=sibling, device_id_type=MESH)
    pl.semaphore_signal(barrier, inc=1, device_id=across, device_id_type=MESH)
    pl.semaphore_wait(barrier, n_chip + 1)

    sent = []

    def remote(src, dst, send, recv, dev):
        return pltpu.make_async_remote_copy(
            src_ref=src, dst_ref=dst, send_sem=send, recv_sem=recv, device_id=dev,
            device_id_type=MESH,
        )

    def start(copy):
        copy.start()
        sent.append(copy)

    cols = [(0, split), (split, inner - split)]
    k_half = inner // 2
    unit_rows = [block] * 4 + [k_half] * 2
    unit_wide = n_chip * block

    def own_view(m, r0, nr):
        c0, nc = cols[m // 2]
        return (gate_hbm, up_hbm)[m % 2].at[pl.ds(r0, nr), pl.ds(c0, nc)]

    def down_lanes(m, slot):
        return pl.ds((m - 4) * unit_wide + slot * block, block)

    def view(m, slot, there, who, r0, nr):
        if m < 4:
            c0, nc = cols[m // 2]
            row = pl.multiple_of((near[slot] * 2 + who) * block + r0, 16)
            return (gate_all, up_all)[m % 2].at[pl.ds(row, nr), pl.ds(c0, nc)]
        row = pl.multiple_of(who * k_half + r0, 16)
        return down_all.at[pl.ds(row, nr), down_lanes(m, slot_of(steps[slot] - there))]

    def piece(m, i, forward):
        nr = unit_rows[m]
        if i < reach - 1:
            return 0, nr
        return (0, nr // 2) if forward else (nr // 2, nr - nr // 2)

    def hop(m, i, forward):
        r0, nr = piece(m, i, forward)
        sign = 1 if forward else -1
        slot = slot_of(-sign * i)
        src = own_view(m, r0, nr) if i == 0 and m < 4 else view(m, slot, 0, core, r0, nr)
        e = 2 * i + (0 if forward else 1)
        start(remote(
            src, view(m, slot, sign, core, r0, nr), ici_send.at[m, e], ici_recv.at[m, e],
            ahead if forward else behind,
        ))

    def landed(m, i, forward):
        r0, nr = piece(m, i, forward)
        sign = 1 if forward else -1
        at = view(m, slot_of(-sign * (i + 1)), 0, core, r0, nr)
        e = 2 * i + (0 if forward else 1)
        remote(at, at, ici_send.at[m, e], ici_recv.at[m, e], ahead).wait_recv()

    def hand(m, slot):
        nr = unit_rows[m]
        at = view(m, slot, 0, core, 0, nr)
        src = own_view(m, 0, nr) if slot == 0 else at
        start(remote(src, at, d2d_send.at[m, slot], d2d_recv.at[m, slot], sibling))

    def handed(m, slot):
        at = view(m, slot, 0, 1 - core, 0, unit_rows[m])
        remote(at, at, d2d_send.at[m, slot], d2d_recv.at[m, slot], sibling).wait_recv()

    def own_lanes(who):
        lane = pl.multiple_of(who * unit_wide, block)
        return down_all.at[:, pl.ds(lane, block)]

    def swap_down(who):
        at = own_lanes(who)
        src = down_hbm if who is core else at
        return remote(src, at, d2d_send.at[4, 0], d2d_recv.at[4, 0], sibling)

    def send_own(m):
        hop(m, 0, True)
        hop(m, 0, False)

    def relay(units, i):
        for m in units:
            landed(m, i, True)
            landed(m, i, False)
            if i + 1 < reach:
                hop(m, i + 1, True)
                hop(m, i + 1, False)
        for m in units:
            if i + 1 < reach:
                hand(m, slot_of(i + 1))
                hand(m, slot_of(-i - 1))
            else:
                hand(m, slot_of(reach))

    for m in range(4):
        send_own(m)
    p_half = proj_hbm.shape[0] // 2
    p_at = pl.ds(pl.multiple_of(core * p_half, p_half), p_half)
    p_to = remote(
        proj_hbm.at[p_at, :], proj_all.at[group, p_at, :], y_send.at[0], y_recv.at[0], across
    )
    start(p_to)
    pairs = [
        (q_hbm, q_ref), (k_hbm, k_ref), (v_hbm, v_ref), (lapse_hbm, lapse_ref),
        (shift_hbm, shift_ref), (docs_hbm, docs_in), (surplus_hbm, surplus_in),
        (switch_hbm, switch_ref), (head_gain_hbm, head_gain_ref),
        (skip_hbm, first), (gain_hbm, gain_ref), (proj_hbm, proj_all.at[group]),
        (down_hbm, own_lanes(core)),
    ] + [(own_view(m, 0, block), view(m, 0, 0, core, 0, block)) for m in range(4)]
    loads = [local_copy(src, dst, load_sem.at[i]) for i, (src, dst) in enumerate(pairs)]
    for copy in loads:
        copy.start()
    for m in range(4):
        hand(m, 0)
    start(swap_down(core))
    for copy in loads[:7]:
        copy.wait()
    for i in range(rows // (2 * SPAN)):
        for j in range(2):
            at = slice(2 * i + j, 2 * i + j + 1)
            lanes = slice(j * SPAN, (j + 1) * SPAN)
            docs_ref[at, :] = docs_in[i : i + 1, lanes].astype(F32)
            surplus_ref[at, :] = surplus_in[i : i + 1, lanes]

    middle = SPAN // 2
    r_i = lax.broadcasted_iota(jnp.int32, (SPAN, SPAN), 0)
    c_i = lax.broadcasted_iota(jnp.int32, (SPAN, SPAN), 1)
    lane_head = lax.broadcasted_iota(jnp.int32, (SPAN, width), 1) // DK
    head_mask = [(lane_head == h).astype(F32) for h in range(heads)]

    def per_head(a):
        return jnp.concatenate([(a * m).astype(BF16) for m in head_mask], axis=0)

    def to_column(row):
        return jnp.sum(jnp.where(r_i == c_i, row, 0.0), axis=1, keepdims=True)

    state[...] = jnp.zeros_like(state)
    total[...] = jnp.zeros_like(total)
    n_block = rows // SPAN

    def attend(b, last):
        lower = r_i >= c_i
        at = pl.ds(pl.multiple_of(b * SPAN, SPAN), SPAN)
        doc_row = docs_ref[pl.ds(b, 1), :]
        doc_col = to_column(doc_row)
        sur_col = to_column(surplus_ref[pl.ds(b, 1), :])
        pre = lapse_ref[at, :].astype(F32) + shift_ref[...]
        ld = (jnp.minimum(pre, 0.0) - jnp.log1p(jnp.exp(-jnp.abs(pre)))) * (
            1.0 / sharpness_factor
        ) + sur_col
        cum = dot1(lower.astype(F32), ld, HIGHEST)
        qb = q_ref[at, :].astype(F32) * DK ** (-0.5)
        kb = k_ref[at, :].astype(F32)
        vb = v_ref[at, :]
        tot = cum[SPAN - 1 : SPAN, :]
        centre = cum[middle : middle + 1, :]
        qd = qb * jnp.exp(cum)
        offset = total[0:1, :]
        qrun[at, :] = (qd * jnp.exp(offset)).astype(BF16)
        qs = qb * jnp.exp(jnp.minimum(cum - centre, LIMIT))
        ks = (kb * jnp.exp(jnp.minimum(centre - cum, LIMIT))).astype(BF16)
        scores = lax.dot_general(
            per_head(qs), ks, (((1,), (1,)), ((), ())), preferred_element_type=F32
        )
        same = (doc_col == doc_row) & lower
        valid = (doc_col == last).astype(F32)
        cross = dot1(per_head(qd), state[...].astype(BF16))
        for h in range(heads):
            piece = slice(h * SPAN, (h + 1) * SPAN)
            lanes = slice(h * DV, (h + 1) * DV)
            masked = jnp.where(same, scores[piece], 0.0).astype(BF16)
            local_out[at, lanes] = dot1(masked, vb[:, lanes]) + cross[piece] * valid
        tail_doc = doc_row[:, SPAN - 1 : SPAN]
        tail_ok = (doc_col == tail_doc).astype(F32)
        kd = (kb * jnp.exp(tot - cum) * tail_ok).astype(BF16)
        update = dot0(kd, vb)
        update = jnp.concatenate(
            [update[h * DK : (h + 1) * DK, h * DV : (h + 1) * DV] for h in range(heads)], axis=0
        )
        keep = (tail_doc == last).astype(F32)
        state[...] = state[...] * (column_of(jnp.exp(tot)) * keep) + update
        total[...] = total[...] + tot
        return tail_doc

    last_own = lax.fori_loop(0, n_block, attend, jnp.full((1, 1), -1.0, F32))

    first_own = docs_ref[0:1, 0:1]
    row8 = lax.broadcasted_iota(jnp.int32, (8, width), 0)

    def small(decay, first_doc, last_doc):
        return jnp.where(row8 == 0, decay, jnp.where(row8 == 1, first_doc, last_doc))

    unbroken = (first_own == last_own).astype(F32)
    st_own[...] = state[...].astype(BF16)
    sm_own[...] = small(jnp.exp(total[0:1, :]) * unbroken, first_own, last_own)

    swap = [
        remote(st_own, st_sib, st_send.at[0], st_recv.at[0], sibling),
        remote(sm_own, sm_sib, st_send.at[1], st_recv.at[1], sibling),
    ]
    for copy in swap:
        start(copy)
    for copy in swap:
        copy.wait_recv()
    low = core == 0
    mine_s, mine_m = st_own[...].astype(F32), sm_own[...]
    sib_s, sib_m = st_sib[...].astype(F32), sm_sib[...]
    lo_s, hi_s = jnp.where(low, mine_s, sib_s), jnp.where(low, sib_s, mine_s)
    lo_m, hi_m = jnp.where(low, mine_m, sib_m), jnp.where(low, sib_m, mine_m)
    joined = (lo_m[2:3, 0:1] == hi_m[1:2, 0:1]).astype(F32)
    hi_decay = hi_m[0:1, :] * joined
    st_cmp[...] = (lo_s * column_of(hi_decay) + hi_s).astype(BF16)
    sm_cmp[...] = small(lo_m[0:1, :] * hi_decay, lo_m[1:2, 0:1], hi_m[2:3, 0:1])

    s_half = width // 2
    s_at = pl.ds(pl.multiple_of(core * s_half, s_half), s_half)
    s_rest = pl.ds(pl.multiple_of((1 - core) * s_half, s_half), s_half)

    def composite(j):
        dev = same_core(lax.rem(chip + j, n_chip))
        return [
            remote(
                st_cmp.at[s_at, :], st_in.at[j - 1, s_at, :],
                st_send.at[2 * j], st_recv.at[2 * j], dev,
            ),
            remote(sm_cmp, sm_in.at[j - 1], st_send.at[2 * j + 1], st_recv.at[2 * j + 1], dev),
        ]

    def other_half(j, at):
        here = st_in.at[j - 1, at, :]
        n = 2 * window + 1 + j
        return remote(here, here, st_send.at[n], st_recv.at[n], sibling)

    for j in range(1, window + 1):

        @pl.when(chip + j < n_chip)
        def _():
            for copy in composite(j):
                copy.start()

    relay((0, 1), 0)
    relay((2, 3), 0)
    for j in range(1, window + 1):

        @pl.when(chip >= j)
        def _():
            for copy in composite(j):
                copy.wait_recv()
            other_half(j, s_at).start()

    for j in range(1, window + 1):

        @pl.when(chip >= j)
        def _():
            other_half(j, s_rest).wait_recv()

    entering = jnp.zeros((width, DV), F32)
    before = jnp.full((1, 1), -1.0, F32)
    for j in range(window, 0, -1):
        valid = chip >= j
        met = jnp.where(valid, sm_in[j - 1], 0.0)
        if j < window:
            linked = (before == met[1:2, 0:1]).astype(F32)
            entering = entering * column_of(met[0:1, :] * linked)
        entering = jnp.where(valid, entering + st_in[j - 1].astype(F32), 0.0)
        before = jnp.where(valid, met[2:3, 0:1], -1.0)
    linked = (before == sib_m[1:2, 0:1]).astype(F32)
    through = entering * column_of(sib_m[0:1, :] * linked) + sib_s
    st_own_f = jnp.where(low, entering, through)
    before = jnp.where(low, before, sib_m[2:3, 0:1])
    state[...] = st_own_f

    for copy in loads[7:9]:
        copy.wait()

    def finish(b, carry):
        at = pl.ds(pl.multiple_of(b * SPAN, SPAN), SPAN)
        reach = (to_column(docs_ref[pl.ds(b, 1), :]) == before).astype(F32)
        qr = qrun[at, :]
        stacked = jnp.concatenate(
            [jnp.where(lane_head == h, qr, jnp.zeros_like(qr)) for h in range(heads)], axis=0
        )
        cross = dot1(stacked, state[...].astype(BF16))
        for h in range(heads):
            lanes = slice(h * DV, (h + 1) * DV)
            attn = local_out[at, lanes] + cross[h * SPAN : (h + 1) * SPAN] * reach
            scaled = (
                attn
                * lax.rsqrt(jnp.mean(attn * attn, axis=-1, keepdims=True) + eps)
                * head_gain_ref[...]
            )
            s = switch_ref[at, lanes].astype(F32)
            gated_all[group, at, lanes] = (scaled * (s / (1.0 + jnp.exp(-s)))).astype(BF16)
        return carry

    lax.fori_loop(0, n_block, finish, 0)
    g_to = remote(
        gated_all.at[group], gated_all.at[group], y_send.at[1], y_recv.at[1], across
    )
    start(g_to)

    p_back = remote(
        proj_all.at[1 - group, p_at, :], proj_all.at[1 - group, p_at, :],
        y_send.at[0], y_recv.at[0], across,
    )
    p_back.wait_recv()
    start(
        remote(
            proj_all.at[1 - group, p_at, :], proj_all.at[1 - group, p_at, :],
            y_send.at[2], y_recv.at[2], sibling,
        )
    )
    relay((0, 1), 1)
    for copy in loads[9:12]:
        copy.wait()
    p_rest = pl.ds(pl.multiple_of((1 - core) * p_half, p_half), p_half)
    remote(
        proj_all.at[1 - group, p_rest, :], proj_all.at[1 - group, p_rest, :],
        y_send.at[2], y_recv.at[2], sibling,
    ).wait_recv()
    remote(
        gated_all.at[1 - group], gated_all.at[1 - group], y_send.at[1], y_recv.at[1], across
    ).wait_recv()
    mix_rows = 256 if rows % 256 == 0 else rows
    mix_cols = 512 if model % 512 == 0 else model

    def mix(r, carry):
        at = pl.ds(pl.multiple_of(r * mix_rows, mix_rows), mix_rows)
        squares = jnp.zeros((mix_rows, 1), F32)
        for c in range(model // mix_cols):
            lanes = slice(c * mix_cols, (c + 1) * mix_cols)
            mixed = jnp.zeros((mix_rows, mix_cols), F32)
            for g in range(2):
                part = jnp.dot(
                    gated_all[g, at, :], proj_all[g, :, lanes], preferred_element_type=F32
                )
                mixed = mixed + part.astype(BF16).astype(F32)
            new = (first[at, lanes].astype(F32) + mixed).astype(BF16)
            first[at, lanes] = new
            wide = new.astype(F32)
            squares = squares + jnp.sum(wide * wide, axis=-1, keepdims=True)
        scale = lax.rsqrt(squares * (1.0 / model) + eps)
        for c in range(model // mix_cols):
            lanes = slice(c * mix_cols, (c + 1) * mix_cols)
            normed[at, lanes] = (
                first[at, lanes].astype(F32) * scale * gain_ref[:, lanes]
            ).astype(BF16)
        return carry

    lax.fori_loop(0, rows // mix_rows, mix, 0)

    relay((2, 3), 1)
    for i in range(2, reach - 1):
        relay((0, 1), i)
        relay((2, 3), i)
    loads[12].wait()
    swap_down(1 - core).wait_recv()
    for m in (4, 5):
        send_own(m)
    relay((0, 1), reach - 1)
    for m in (0, 1):
        loads[13 + m].wait()
        for slot in range(n_chip):
            handed(m, slot)
    def expand(t, carry):
        lanes = pl.ds(pl.multiple_of(t * TILE, TILE), TILE)
        g = jnp.dot(normed[...], gate_all[:, lanes], preferred_element_type=F32)
        u = jnp.dot(normed[...], up_all[:, lanes], preferred_element_type=F32)
        hidden[:, lanes] = (g / (1.0 + jnp.exp(-g)) * u).astype(BF16)
        return carry

    lax.fori_loop(0, split // TILE, expand, 0)

    relay((2, 3), reach - 1)
    relay((4,), 0)
    for m in (2, 3):
        loads[13 + m].wait()
        for slot in range(n_chip):
            handed(m, slot)
    lax.fori_loop(split // TILE, inner // TILE, expand, 0)

    own_rows = pl.ds(pl.multiple_of(group * half, half), half)

    def reduce_copy(m, lo, hi):
        lanes = pl.ds((m - 4) * unit_wide + lo * block, (hi - lo) * block)
        n = (m - 4) * n_chip + lo
        return remote(
            normed.at[:half, lanes], recv_buf.at[:, lanes], red_send.at[n], red_recv.at[n], across
        )

    def shrink(m, lo, hi):
        lanes = slice((m - 4) * unit_wide + lo * block, (m - 4) * unit_wide + hi * block)
        a = jnp.dot(hidden[:half], down_all[:, lanes], preferred_element_type=F32)
        b = jnp.dot(hidden[half:], down_all[:, lanes], preferred_element_type=F32)
        normed[:half, lanes] = jnp.where(group == 0, b, a).astype(BF16)
        normed[half:, lanes] = jnp.where(group == 0, a, b).astype(BF16)
        start(reduce_copy(m, lo, hi))

    def settle(m, lo, hi):
        reduce_copy(m, lo, hi).wait_recv()
        for slot in range(lo, hi):
            at = slice((m - 4) * unit_wide + slot * block, (m - 4) * unit_wide + (slot + 1) * block)
            lane = (near[slot] * 2 + m - 4) * block
            lanes = pl.ds(pl.multiple_of(lane, block), block)
            ffn = normed[half:, at].astype(F32) + recv_buf[:, at].astype(F32)
            out_ref[:, lanes] = (first[own_rows, lanes].astype(F32) + 0.5 * ffn).astype(BF16)

    def handed_down(m, lo, hi):
        for slot in range(lo, hi):
            handed(m, slot)

    shrink(4, 0, 1)
    shrink(5, 0, 1)
    relay((5,), 0)
    waiting = [(4, 0, 1), (5, 0, 1)]
    for i in range(1, reach):
        for m in (4, 5):
            if i > 1:
                relay((m,), i - 1)
            handed_down(m, 2 * i - 1, 2 * i + 1)
            shrink(m, 2 * i - 1, 2 * i + 1)
            settle(*waiting.pop(0))
            waiting.append((m, 2 * i - 1, 2 * i + 1))
    for m in (4, 5):
        relay((m,), reach - 1)
        handed_down(m, n_chip - 1, n_chip)
        shrink(m, n_chip - 1, n_chip)
        waiting.append((m, n_chip - 1, n_chip))
        settle(*waiting.pop(0))
    for last in waiting:
        settle(*last)
    for copy in sent:
        copy.wait_send()
    for j in range(1, window + 1):

        @pl.when(chip + j < n_chip)
        def _():
            for copy in composite(j):
                copy.wait_send()

        @pl.when(chip >= j)
        def _():
            other_half(j, s_at).wait_send()


def fused_per_device(
    skip_connection_stream,
    probing_vectors,
    addressing_vectors,
    mapped_payloads,
    emission_switch,
    lapse_preactivation,
    lapse_shift_entries,
    surplus_attenuation_terms,
    passage_label_per_token,
    attention_group_rescaler,
    emission_projector,
    perceptron_rescaler,
    switching_projector,
    widening_projector,
    shrinking_projector,
):
    rows, width = probing_vectors.shape
    group_w = mapped_payloads.shape[1]
    model = skip_connection_stream.shape[1]
    block, inner = switching_projector.shape
    n_sp, n_tp = lax.axis_size("sp"), lax.axis_size("tp")
    n_chip = n_sp // 2
    window = min(pl.cdiv(DOC_MOST, 2 * rows), n_chip - 1)
    tiles = inner // TILE
    split = TILE * pl.cdiv(tiles * 3, 5)
    half = rows // 2
    docs = passage_label_per_token.reshape(-1, 2 * SPAN)
    surplus = surplus_attenuation_terms.reshape(-1, 2 * SPAN)
    DMA = pltpu.SemaphoreType.DMA
    hbm = pl.BlockSpec(memory_space=pl.ANY)
    plan = (n_chip, window, split)
    return pl.pallas_call(
        functools.partial(fused_kernel, plan),
        out_shape=pltpu.VMEM((half, model), BF16),
        in_specs=[hbm] * 15,
        out_specs=vmem(1)[0],
        scratch_shapes=[
            pltpu.VMEM((1, width), F32),
            pltpu.VMEM((rows // (2 * SPAN), 2 * SPAN), jnp.int32),
            pltpu.VMEM((rows // (2 * SPAN), 2 * SPAN), F32),
            pltpu.VMEM((1, DV), F32),
            pltpu.VMEM((1, model), F32),
            pltpu.VMEM((rows // SPAN, SPAN), F32),
            pltpu.VMEM((rows // SPAN, SPAN), F32),
            pltpu.VMEM((model, inner), BF16),
            pltpu.VMEM((model, inner), BF16),
            pltpu.VMEM((inner, model), BF16),
            pltpu.VMEM((n_tp, group_w, model), BF16),
            pltpu.VMEM((n_tp, rows, group_w), BF16),
            pltpu.VMEM((rows, model), BF16),
            pltpu.VMEM((rows, model), BF16),
            pltpu.VMEM((rows, inner), BF16),
            pltpu.VMEM((rows, width), BF16),
            pltpu.VMEM((rows, width), BF16),
            pltpu.VMEM((rows, group_w), BF16),
            pltpu.VMEM((rows, group_w), BF16),
            pltpu.VMEM((rows, width), BF16),
            pltpu.VMEM((rows, group_w), F32),
            pltpu.VMEM((rows, width), BF16),
            pltpu.VMEM((width, DV), F32),
            pltpu.VMEM((8, width), F32),
            pltpu.VMEM((width, DV), BF16),
            pltpu.VMEM((8, width), F32),
            pltpu.VMEM((width, DV), BF16),
            pltpu.VMEM((8, width), F32),
            pltpu.VMEM((width, DV), BF16),
            pltpu.VMEM((8, width), F32),
            pltpu.VMEM((window, width, DV), BF16),
            pltpu.VMEM((window, 8, width), F32),
            pltpu.VMEM((half, model), BF16),
            DMA((17,)),
            DMA((6, n_chip)),
            DMA((6, n_chip)),
            DMA((6, n_chip)),
            DMA((6, n_chip)),

            DMA((3,)),
            DMA((3,)),
            DMA((3 * window + 2,)),
            DMA((3 * window + 2,)),
            DMA((2 * n_chip,)),
            DMA((2 * n_chip,)),
        ],
        compiler_params=pltpu.CompilerParams(
            collective_id=0, has_side_effects=True, vmem_limit_bytes=62_000_000
        ),
        cost_estimate=pl.CostEstimate(
            flops=30_000_000_000, bytes_accessed=20_000_000, transcendentals=0
        ),
        name="fused_layer",
    )(
        skip_connection_stream,
        probing_vectors,
        addressing_vectors,
        mapped_payloads,
        emission_switch,
        lapse_preactivation,
        emission_projector,
        switching_projector,
        widening_projector,
        shrinking_projector,
        lapse_shift_entries[None, :],
        docs,
        surplus,
        attention_group_rescaler[None, :],
        perceptron_rescaler[None, :],
    )


def fits_fused(mesh, arrays):
    n_sp, n_tp = mesh.shape["sp"], mesh.shape["tp"]
    gate = arrays[12]
    block, inner = gate.shape[0] // n_sp, gate.shape[1] // n_tp
    even = n_sp % 8 == 0 and n_tp == 2
    return even and block % 128 == 0 and inner % TILE == 0 and 6 * gate.size // n_tp < 2**25 * 3 // 2


def solution(mesh):
    placed = (
        P("sp", None),
        P("sp", "tp"),
        P("sp", "tp"),
        P("sp", "tp"),
        P("sp", "tp"),
        P("sp", "tp"),
        P("tp"),
        P("sp"),
        P("sp"),
        P(),
        P("tp", None),
        P(),
        P("sp", "tp"),
        P("sp", "tp"),
        P("tp", "sp"),
    )

    def layer(*arrays):
        body = fused_per_device if fits_fused(mesh, arrays) else per_device
        return jax.shard_map(
            body, mesh=mesh, in_specs=placed, out_specs=P(("sp", "tp"), None), check_vma=False
        )(*arrays)

    return layer
```

```python
import functools

import jax
import jax.numpy as jnp
from jax import lax
from jax.experimental import pallas as pl
from jax.experimental.pallas import tpu as pltpu
from jax.sharding import PartitionSpec as P

DK = 64
DV = 128
BLOCK = 64
LIMIT = 80.0

eps = 1e-06
sharpness_factor = 16.0
HIGHEST = lax.Precision.HIGHEST
F32 = jnp.float32
BF16 = jnp.bfloat16


def dot0(a, b, precision=None):
    return lax.dot_general(
        a, b, (((0,), (0,)), ((), ())), precision=precision, preferred_element_type=F32
    )


def dot1(a, b, precision=None):
    return lax.dot_general(
        a, b, (((1,), (0,)), ((), ())), precision=precision, preferred_element_type=F32
    )


def local_pass(
    q_ref, k_ref, v_ref, lapse_ref, shift_ref, surplus_ref, doc_col_ref, doc_row_ref,
    out_ref, qrun_ref, state_ref, total_ref,
):
    length, width = q_ref.shape
    heads = width // DK
    span = BLOCK
    middle = span // 2
    rows = lax.broadcasted_iota(jnp.int32, (span, span), 0)
    cols = lax.broadcasted_iota(jnp.int32, (span, span), 1)
    lower = rows >= cols
    tril = lower.astype(F32)
    ones = jnp.ones((span, DV), F32)
    lane_head = lax.broadcasted_iota(jnp.int32, (span, width), 1) // DK
    head_mask = [(lane_head == h).astype(F32) for h in range(heads)]

    def per_head(a):
        return jnp.concatenate([(a * m).astype(BF16) for m in head_mask], axis=0)

    state = None
    offset = jnp.zeros((1, width), F32)
    for b in range(length // span):
        at = pl.ds(b * span, span)
        pre = lapse_ref[at, :].astype(F32) + shift_ref[...]
        ld = (jnp.minimum(pre, 0.0) - jnp.log1p(jnp.exp(-jnp.abs(pre)))) * (
            1.0 / sharpness_factor
        ) + surplus_ref[at, :]
        cum = dot1(tril, ld, HIGHEST)
        q = q_ref[at, :].astype(F32) * DK ** (-0.5)
        k = k_ref[at, :].astype(F32)
        v = v_ref[at, :]
        doc_col = doc_col_ref[at, :]
        doc_row = doc_row_ref[b : b + 1, :]
        tot = cum[span - 1 : span, :]
        centre = cum[middle : middle + 1, :]
        decayed = jnp.exp(cum)
        qd = q * decayed
        qrun_ref[at, :] = (qd * jnp.exp(offset)).astype(BF16)
        qs = q * jnp.exp(jnp.minimum(cum - centre, LIMIT))
        ks = (k * jnp.exp(jnp.minimum(centre - cum, LIMIT))).astype(BF16)
        scores = lax.dot_general(
            per_head(qs), ks, (((1,), (1,)), ((), ())), preferred_element_type=F32
        )
        same = (doc_col == doc_row) & lower
        if b > 0:
            last = doc_col_ref[b * span - 1 : b * span, :]
            valid = (doc_col == last).astype(F32)
            cross = dot1(per_head(qd), state.astype(BF16))
        for h in range(heads):
            piece = slice(h * span, (h + 1) * span)
            lanes = slice(h * DV, (h + 1) * DV)
            masked = jnp.where(same, scores[piece], 0.0).astype(BF16)
            res = dot1(masked, v[:, lanes])
            if b > 0:
                res = res + cross[piece] * valid
            out_ref[at, lanes] = res
        tail_doc = doc_col[span - 1 : span, :]
        tail_ok = (doc_col == tail_doc).astype(F32)
        kd = (k * jnp.exp(tot - cum) * tail_ok).astype(BF16)
        update = dot0(kd, v)
        update = jnp.concatenate(
            [update[h * DK : (h + 1) * DK, h * DV : (h + 1) * DV] for h in range(heads)], axis=0
        )
        if b > 0:
            keep = (tail_doc == last).astype(F32)
            state = state * (jnp.exp(dot0(ld, ones, HIGHEST)) * keep) + update
        else:
            state = update
        offset = offset + tot
    state_ref[...] = state
    total_ref[...] = offset


def finish_pass(out_ref, qrun_ref, entering_ref, reaches_ref, switch_ref, gain_ref, gated_ref):
    length, width = qrun_ref.shape
    heads = width // DK
    rows = 256 if length % 256 == 0 else length
    lane_head = lax.broadcasted_iota(jnp.int32, (rows, width), 1) // DK
    for r in range(length // rows):
        at = pl.ds(r * rows, rows)
        q = qrun_ref[at, :]
        reaches = reaches_ref[at, :]
        for h in range(heads):
            lanes = slice(h * DV, (h + 1) * DV)
            qh = jnp.where(lane_head == h, q, jnp.zeros_like(q))
            attn = out_ref[at, lanes] + dot1(qh, entering_ref[...]) * reaches
            normed = (
                attn
                * lax.rsqrt(jnp.mean(attn * attn, axis=-1, keepdims=True) + eps)
                * gain_ref[...]
            )
            s = switch_ref[at, lanes].astype(F32)
            gated_ref[at, lanes] = (normed * (s / (1.0 + jnp.exp(-s)))).astype(BF16)


def rms_rows(rows, gain):
    wide = rows.astype(F32)
    return (wide * lax.rsqrt(jnp.mean(wide * wide, axis=-1, keepdims=True) + eps) * gain).astype(
        BF16
    )


def ring_orders(n_sp):
    chips = n_sp // 2
    return list(range(0, chips, 2)) + list(range(1, chips, 2))[::-1]


def ring_pairs(n_sp, step):
    ring = ring_orders(n_sp)
    count = len(ring)
    return [
        (2 * ring[i] + core, 2 * ring[(i + step) % count] + core)
        for i in range(count)
        for core in (0, 1)
    ]


def swap_cores(a, n_sp):
    return lax.ppermute(a, "sp", [(i, i ^ 1) for i in range(n_sp)])


def ring_start(own, n_sp):
    return (
        lax.ppermute(own, "sp", ring_pairs(n_sp, 1)),
        lax.ppermute(own, "sp", ring_pairs(n_sp, -1)),
    )


def ring_rest(first, n_sp, axis):
    behind, ahead = [first[0]], [first[1]]
    count = n_sp // 2
    for _ in range((count - 1) // 2 - 1):
        behind.append(lax.ppermute(behind[-1], "sp", ring_pairs(n_sp, 1)))
        ahead.append(lax.ppermute(ahead[-1], "sp", ring_pairs(n_sp, -1)))
    size = first[0].shape[axis] // 2
    low = lax.slice_in_dim(behind[-1], 0, size, axis=axis)
    high = lax.slice_in_dim(ahead[-1], size, 2 * size, axis=axis)
    low = lax.ppermute(low, "sp", ring_pairs(n_sp, 1))
    high = lax.ppermute(high, "sp", ring_pairs(n_sp, -1))
    return behind, ahead, (low, high)


def vmem(n):
    return [pl.BlockSpec(memory_space=pltpu.VMEM)] * n


def per_device(
    skip_connection_stream,
    probing_vectors,
    addressing_vectors,
    mapped_payloads,
    emission_switch,
    lapse_preactivation,
    lapse_shift_entries,
    surplus_attenuation_terms,
    passage_label_per_token,
    attention_group_rescaler,
    emission_projector,
    perceptron_rescaler,
    switching_projector,
    widening_projector,
    shrinking_projector,
):
    rows_here, width = probing_vectors.shape
    heads = width // DK
    n_sp, n_tp = lax.axis_size("sp"), lax.axis_size("tp")
    place, group = lax.axis_index("sp"), lax.axis_index("tp")
    docs = passage_label_per_token

    def to_later(a, step):
        return lax.ppermute(a, "tp", [(i, (i + step) % n_tp) for i in range(n_tp)])

    both_w = jnp.concatenate([switching_projector, widening_projector], axis=1)
    both_first = ring_start(both_w, n_sp)
    down_first = ring_start(shrinking_projector, n_sp)
    projectors = [emission_projector] + [to_later(emission_projector, s) for s in range(1, n_tp)]

    local_out, qrun, state, total = pl.pallas_call(
        local_pass,
        out_shape=(
            jax.ShapeDtypeStruct((rows_here, heads * DV), F32),
            jax.ShapeDtypeStruct((rows_here, width), BF16),
            jax.ShapeDtypeStruct((width, DV), F32),
            jax.ShapeDtypeStruct((1, width), F32),
        ),
        in_specs=vmem(8),
        out_specs=tuple(vmem(4)),
        cost_estimate=pl.CostEstimate(
            flops=40_000_000_000, bytes_accessed=6_000_000, transcendentals=0
        ),
        name="local_pass",
    )(
        probing_vectors,
        addressing_vectors,
        mapped_payloads,
        lapse_preactivation,
        lapse_shift_entries[None, :],
        surplus_attenuation_terms[:, None],
        docs[:, None],
        docs.reshape(-1, BLOCK),
    )

    unbroken = (docs[0] == docs[-1]).astype(F32)
    ends = jnp.stack([docs[0], docs[-1]]).astype(BF16)
    small = jnp.concatenate([(jnp.exp(total[0]) * unbroken).astype(BF16), ends])
    tail_rows = 16 * pl.cdiv(small.size, 16 * DV)
    small = jnp.pad(small, (0, tail_rows * DV - small.size)).reshape(tail_rows, DV)
    packed = jnp.concatenate([state.astype(BF16), small], axis=0)
    half = (width + tail_rows) // 2
    first_half = lax.all_gather(packed[:half], "sp")
    packed, first_half = lax.optimization_barrier((packed, first_half))
    second_half = lax.all_gather(packed[half:], "sp")
    second_half, both_first = lax.optimization_barrier((second_half, both_first))
    packed = jnp.concatenate([first_half, second_half], axis=1)
    behind, ahead, opposite = ring_rest(both_first, n_sp, 1)
    down_first, opposite = lax.optimization_barrier((down_first, opposite))
    down_behind, down_ahead, down_opposite = ring_rest(down_first, n_sp, 0)

    ring = jnp.asarray(ring_orders(n_sp), jnp.int32)
    count = n_sp // 2
    spot = jnp.argmax(ring == place // 2)
    core = place % 2

    def chip_at(steps_behind):
        return ring[(spot - steps_behind + count) % count]

    chips = [chip_at(0)]
    chips += [chip_at(d + 1) for d in range(len(behind))]
    chips += [chip_at(-d - 1) for d in range(len(ahead))]
    chips += [chip_at(count // 2)]
    owners = [2 * c + core for c in chips] + [2 * c + 1 - core for c in chips]
    lows, highs = opposite
    here = [both_w] + behind + ahead + [jnp.concatenate([lows, highs], axis=1)]
    there = [swap_cores(a, n_sp) for a in [both_w] + behind + ahead]
    there += [jnp.concatenate([swap_cores(lows, n_sp), swap_cores(highs, n_sp)], axis=1)]
    hidden_width = switching_projector.shape[1]
    gate_w = jnp.concatenate([a[:, :hidden_width] for a in here + there], axis=0)
    up_w = jnp.concatenate([a[:, hidden_width:] for a in here + there], axis=0)
    down_here = [shrinking_projector] + down_behind + down_ahead
    down_there = [swap_cores(a, n_sp) for a in down_here]
    states = packed[:, :width]
    smalls = packed[:, width:].reshape(n_sp, -1).astype(F32)
    decays, first_doc, last_doc = smalls[:, :width], smalls[:, width], smalls[:, width + 1]
    before = jnp.concatenate([jnp.full((1,), -1.0, F32), last_doc[:-1]])
    decays = decays * (before == first_doc).astype(F32)[:, None]
    entering = jnp.zeros((width, DV), F32)
    for j in range(n_sp):
        entering = jnp.where(
            j < place, entering * decays[j][:, None] + states[j].astype(F32), entering
        )
    reaches = (docs.astype(F32) == before[place]).astype(F32)

    gated = pl.pallas_call(
        finish_pass,
        out_shape=jax.ShapeDtypeStruct((rows_here, heads * DV), BF16),
        in_specs=vmem(6),
        out_specs=vmem(1)[0],
        cost_estimate=pl.CostEstimate(
            flops=5_000_000_000, bytes_accessed=5_000_000, transcendentals=0
        ),
        name="finish_pass",
    )(
        local_out,
        qrun,
        entering.astype(BF16),
        reaches[:, None],
        emission_switch,
        attention_group_rescaler[None, :],
    )

    gateds = [gated] + [to_later(gated, s) for s in range(1, n_tp)]
    mixed = jnp.zeros((), F32)
    for rows, weight in zip(gateds, projectors):
        part = jnp.dot(rows, weight, preferred_element_type=F32).astype(BF16)
        mixed = mixed + part.astype(F32)
    first_all = (skip_connection_stream.astype(F32) + mixed).astype(BF16)
    normed = rms_rows(first_all, perceptron_rescaler)
    block = switching_projector.shape[0]

    def columns(a, owner):
        return lax.dynamic_slice_in_dim(a, owner * block, block, 1)

    ringed = jnp.concatenate([columns(normed, owner) for owner in owners], axis=1)
    gate = jnp.dot(ringed, gate_w, preferred_element_type=F32)
    upper = jnp.dot(ringed, up_w, preferred_element_type=F32)
    hidden = (jax.nn.silu(gate) * upper).astype(BF16)

    share = rows_here // n_tp

    def share_of(a, owner):
        return lax.dynamic_slice_in_dim(a, owner * share, share, 0)

    def reduced(weight):
        def down(owner):
            return jnp.dot(share_of(hidden, owner), weight, preferred_element_type=F32).astype(BF16)

        arrived = [to_later(down((group + s) % n_tp), s) for s in range(1, n_tp)]
        total = down(group).astype(F32)
        for part in arrived:
            total = total + part.astype(F32)
        return total

    late_here = jnp.concatenate(down_opposite, axis=0)
    late_there = jnp.concatenate([swap_cores(a, n_sp) for a in down_opposite], axis=0)
    near = (len(down_here) + 1) // 2
    order = [0] + [i + 1 + j * len(down_behind) for i in range(len(down_behind)) for j in (0, 1)]
    groups = [order[:near], order[near:], [len(down_here)]]
    down_here, down_there = down_here + [late_here], down_there + [late_there]
    first_own = share_of(first_all, group)
    out = first_own
    for members in groups:
        weight = jnp.concatenate(
            [down_here[i] for i in members] + [down_there[i] for i in members], axis=1
        )
        whose = [owners[i] for i in members] + [owners[len(chips) + i] for i in members]
        total = reduced(weight)
        for i, owner in enumerate(whose):
            start = (0, owner * block)
            piece = total[:, i * block : (i + 1) * block]
            base = lax.dynamic_slice(first_own, start, (share, block)).astype(F32)
            out = lax.dynamic_update_slice(out, (base + 0.5 * piece).astype(BF16), start)
    return out


MESH = pl.DeviceIdType.MESH
SPAN = BLOCK
TILE = 256
DOC_MOST = 6144


def local_copy(src, dst, sem):
    return pltpu.make_async_copy(src, dst, sem)


def column_of(row):
    first = lax.broadcasted_iota(jnp.int32, (8, row.shape[1]), 0) == 0
    return dot0(jnp.where(first, row, 0.0), jnp.ones((8, DV), F32), HIGHEST)


def ring_chip(spot, n_chip):
    return jnp.where(spot < n_chip // 2, 2 * spot, 2 * (n_chip - 1 - spot) + 1)


def ring_spot(chip, n_chip):
    return jnp.where(chip % 2 == 0, chip // 2, n_chip - 1 - chip // 2)


def fused_kernel(
    plan,
    skip_hbm, q_hbm, k_hbm, v_hbm, switch_hbm, lapse_hbm, proj_hbm, gate_hbm, up_hbm, down_hbm,
    shift_hbm, docs_hbm, surplus_hbm, head_gain_hbm, gain_hbm,
    out_ref,
    shift_ref, docs_in, surplus_in, head_gain_ref, gain_ref, docs_ref, surplus_ref,
    gate_all, up_all, down_all, proj_all, gated_all, first, normed, hidden,
    q_ref, k_ref, v_ref, switch_ref, lapse_ref, local_out, qrun, state, total,
    st_own, sm_own, st_sib, sm_sib, st_cmp, sm_cmp, st_side, sm_side, st_plane, sm_plane,
    st_in, sm_in, st_all,
    recv_buf,
    load_sem, ici_send, ici_recv, d2d_send, d2d_recv,
    y_send, y_recv, st_send, st_recv, red_send, red_recv,
):
    n_chip, window, split = plan
    rows, width = q_ref.shape
    heads = width // DK
    group_w = heads * DV
    model = normed.shape[1]
    inner = hidden.shape[1]
    block = gate_hbm.shape[0]
    half = rows // 2

    place = lax.axis_index("sp")
    group = lax.axis_index("tp")
    core = lax.rem(place, 2)
    chip = place // 2
    reach = n_chip // 2
    spot = ring_spot(chip, n_chip)
    steps = [0] + [d for i in range(1, reach) for d in (i, -i)] + [reach]
    near = [ring_chip(lax.rem(spot + d + n_chip, n_chip), n_chip) for d in steps]
    sibling = {"sp": chip * 2 + 1 - core}
    across = {"tp": 1 - group}

    def same_core(c):
        return {"sp": c * 2 + core}

    ahead, behind = same_core(near[1]), same_core(near[2])

    def slot_of(d):
        return steps.index(d if -reach < d else d + n_chip)

    barrier = pltpu.get_barrier_semaphore()
    for j in range(1, n_chip):
        pl.semaphore_signal(
            barrier, inc=1, device_id=same_core(lax.rem(chip + j, n_chip)), device_id_type=MESH
        )
    pl.semaphore_signal(barrier, inc=1, device_id=sibling, device_id_type=MESH)
    pl.semaphore_signal(barrier, inc=1, device_id=across, device_id_type=MESH)
    pl.semaphore_wait(barrier, n_chip + 1)

    sent = []

    def remote(src, dst, send, recv, dev):
        return pltpu.make_async_remote_copy(
            src_ref=src, dst_ref=dst, send_sem=send, recv_sem=recv, device_id=dev,
            device_id_type=MESH,
        )

    def start(copy):
        copy.start()
        sent.append(copy)

    cols = [(0, split), (split, inner - split)]
    k_half = inner // 2
    unit_rows = [block] * 4 + [k_half] * 2
    unit_wide = n_chip * block

    def own_view(m, r0, nr):
        c0, nc = cols[m // 2]
        return (gate_hbm, up_hbm)[m % 2].at[pl.ds(r0, nr), pl.ds(c0, nc)]

    def down_lanes(m, slot):
        return pl.ds((m - 4) * unit_wide + slot * block, block)

    def view(m, slot, there, who, r0, nr):
        if m < 4:
            c0, nc = cols[m // 2]
            row = pl.multiple_of((near[slot] * 2 + who) * block + r0, 16)
            return (gate_all, up_all)[m % 2].at[pl.ds(row, nr), pl.ds(c0, nc)]
        row = pl.multiple_of(who * k_half + r0, 16)
        return down_all.at[pl.ds(row, nr), down_lanes(m, slot_of(steps[slot] - there))]

    def piece(m, i, forward):
        nr = unit_rows[m]
        if i < reach - 1:
            return 0, nr
        return (0, nr // 2) if forward else (nr // 2, nr - nr // 2)

    def joint(m):
        return m // 2 if m < 4 else m - 2

    def kind(m):
        return m % 2 if m < 4 else 2

    def hop(m, i, forward):
        r0, nr = piece(m, i, forward)
        sign = 1 if forward else -1
        slot = slot_of(-sign * i)
        src = own_view(m, r0, nr) if i == 0 and m < 4 else view(m, slot, 0, core, r0, nr)
        remote(
            src, view(m, slot, sign, core, r0, nr), ici_send.at[kind(m)], ici_recv.at[joint(m), i],
            ahead if forward else behind,
        ).start()

    def bytes_of(m, units):
        if m < 4:
            c0, nc = cols[m // 2]
            return gate_all.at[pl.ds(0, units * block), pl.ds(c0, nc)]
        return down_all.at[pl.ds(0, k_half), pl.ds(0, units * block)]

    def await_bytes(at, sem):
        remote(at, at, sem, sem, ahead).wait_recv()

    def landed(m, i):
        n = (2 if m < 4 else 1) * (2 if i + 1 < reach else 1)
        await_bytes(bytes_of(m, n), ici_recv.at[joint(m), i])

    def hand(m, slot):
        nr = unit_rows[m]
        at = view(m, slot, 0, core, 0, nr)
        src = own_view(m, 0, nr) if slot == 0 else at
        step = (slot + 1) // 2 if m >= 4 else 0
        remote(
            src, at, d2d_send.at[kind(m)], d2d_recv.at[joint(m), step], sibling
        ).start()

    def handed_part(m):
        await_bytes(bytes_of(m, 2 * n_chip), d2d_recv.at[joint(m), 0])

    def handed_down(m, i):
        n = 2 if i < reach else 1
        await_bytes(bytes_of(m, n), d2d_recv.at[joint(m), i])

    def all_sent():
        for n in range(2):
            at = (gate_all, up_all)[n].at[pl.ds(0, (n_chip - 1) * block), :]
            remote(at, at, ici_send.at[n], ici_send.at[n], ahead).wait_send()
            at = (gate_all, up_all)[n].at[pl.ds(0, n_chip * block), :]
            remote(at, at, d2d_send.at[n], d2d_send.at[n], sibling).wait_send()
        at = down_all.at[:, pl.ds(0, (n_chip - 1) * block)]
        remote(at, at, ici_send.at[2], ici_send.at[2], ahead).wait_send()
        remote(at, at, d2d_send.at[2], d2d_send.at[2], sibling).wait_send()

    def own_lanes(who):
        lane = pl.multiple_of(who * unit_wide, block)
        return down_all.at[:, pl.ds(lane, block)]

    def swap_down(who):
        at = own_lanes(who)
        src = down_hbm if who is core else at
        return remote(src, at, d2d_send.at[3], d2d_recv.at[2, 0], sibling)

    def send_own(m):
        hop(m, 0, True)
        hop(m, 0, False)

    def relay(units, i):
        landed(units[0], i)
        for m in units:
            if i + 1 < reach:
                hop(m, i + 1, True)
                hop(m, i + 1, False)
        for m in units:
            if i + 1 < reach:
                hand(m, slot_of(i + 1))
                hand(m, slot_of(-i - 1))
            else:
                hand(m, slot_of(reach))

    for m in range(2):
        send_own(m)
    p_half = proj_hbm.shape[0] // 2
    p_at = pl.ds(pl.multiple_of(core * p_half, p_half), p_half)
    p_to = remote(
        proj_hbm.at[p_at, :], proj_all.at[group, p_at, :], y_send.at[0], y_recv.at[0], across
    )
    start(p_to)
    pairs = [
        (q_hbm, q_ref), (k_hbm, k_ref), (v_hbm, v_ref), (lapse_hbm, lapse_ref),
        (shift_hbm, shift_ref), (docs_hbm, docs_in), (surplus_hbm, surplus_in),
        (switch_hbm, switch_ref), (head_gain_hbm, head_gain_ref),
        (skip_hbm, first), (gain_hbm, gain_ref), (proj_hbm, proj_all.at[group]),
        (down_hbm, own_lanes(core)),
    ] + [(own_view(m, 0, block), view(m, 0, 0, core, 0, block)) for m in range(4)]
    loads = [local_copy(src, dst, load_sem.at[i]) for i, (src, dst) in enumerate(pairs)]
    for copy in loads:
        copy.start()
    for m in range(4):
        hand(m, 0)
    start(swap_down(core))
    for copy in loads[:7]:
        copy.wait()
    for i in range(rows // (2 * SPAN)):
        for j in range(2):
            at = slice(2 * i + j, 2 * i + j + 1)
            lanes = slice(j * SPAN, (j + 1) * SPAN)
            docs_ref[at, :] = docs_in[i : i + 1, lanes].astype(F32)
            surplus_ref[at, :] = surplus_in[i : i + 1, lanes]

    middle = SPAN // 2
    r_i = lax.broadcasted_iota(jnp.int32, (SPAN, SPAN), 0)
    c_i = lax.broadcasted_iota(jnp.int32, (SPAN, SPAN), 1)
    lane_head = lax.broadcasted_iota(jnp.int32, (SPAN, width), 1) // DK
    head_mask = [(lane_head == h).astype(F32) for h in range(heads)]

    def per_head(a):
        return jnp.concatenate([(a * m).astype(BF16) for m in head_mask], axis=0)

    def to_column(row):
        return jnp.sum(jnp.where(r_i == c_i, row, 0.0), axis=1, keepdims=True)

    state[...] = jnp.zeros_like(state)
    total[...] = jnp.zeros_like(total)
    n_block = rows // SPAN

    def attend(b, last):
        lower = r_i >= c_i
        at = pl.ds(pl.multiple_of(b * SPAN, SPAN), SPAN)
        doc_row = docs_ref[pl.ds(b, 1), :]
        doc_col = to_column(doc_row)
        sur_col = to_column(surplus_ref[pl.ds(b, 1), :])
        pre = lapse_ref[at, :].astype(F32) + shift_ref[...]
        ld = (jnp.minimum(pre, 0.0) - jnp.log1p(jnp.exp(-jnp.abs(pre)))) * (
            1.0 / sharpness_factor
        ) + sur_col
        cum = dot1(lower.astype(F32), ld, HIGHEST)
        qb = q_ref[at, :].astype(F32) * DK ** (-0.5)
        kb = k_ref[at, :].astype(F32)
        vb = v_ref[at, :]
        tot = cum[SPAN - 1 : SPAN, :]
        centre = cum[middle : middle + 1, :]
        qd = qb * jnp.exp(cum)
        offset = total[0:1, :]
        qrun[at, :] = (qd * jnp.exp(offset)).astype(BF16)
        qs = qb * jnp.exp(jnp.minimum(cum - centre, LIMIT))
        ks = (kb * jnp.exp(jnp.minimum(centre - cum, LIMIT))).astype(BF16)
        scores = lax.dot_general(
            per_head(qs), ks, (((1,), (1,)), ((), ())), preferred_element_type=F32
        )
        same = (doc_col == doc_row) & lower
        valid = (doc_col == last).astype(F32)
        cross = dot1(per_head(qd), state[...].astype(BF16))
        for h in range(heads):
            piece = slice(h * SPAN, (h + 1) * SPAN)
            lanes = slice(h * DV, (h + 1) * DV)
            masked = jnp.where(same, scores[piece], 0.0).astype(BF16)
            local_out[at, lanes] = dot1(masked, vb[:, lanes]) + cross[piece] * valid
        tail_doc = doc_row[:, SPAN - 1 : SPAN]
        tail_ok = (doc_col == tail_doc).astype(F32)
        kd = (kb * jnp.exp(tot - cum) * tail_ok).astype(BF16)
        update = dot0(kd, vb)
        update = jnp.concatenate(
            [update[h * DK : (h + 1) * DK, h * DV : (h + 1) * DV] for h in range(heads)], axis=0
        )
        keep = (tail_doc == last).astype(F32)
        state[...] = state[...] * (column_of(jnp.exp(tot)) * keep) + update
        total[...] = total[...] + tot
        return tail_doc

    last_own = lax.fori_loop(0, n_block, attend, jnp.full((1, 1), -1.0, F32))

    first_own = docs_ref[0:1, 0:1]
    row8 = lax.broadcasted_iota(jnp.int32, (8, width), 0)

    def small(decay, first_doc, last_doc):
        return jnp.where(row8 == 0, decay, jnp.where(row8 == 1, first_doc, last_doc))

    unbroken = (first_own == last_own).astype(F32)
    st_own[...] = state[...].astype(BF16)
    sm_own[...] = small(jnp.exp(total[0:1, :]) * unbroken, first_own, last_own)

    swap = [
        remote(st_own, st_sib, st_send.at[0], st_recv.at[0], sibling),
        remote(sm_own, sm_sib, st_send.at[1], st_recv.at[1], sibling),
    ]
    for copy in swap:
        start(copy)
    for copy in swap:
        copy.wait_recv()
    low = core == 0
    mine_s, mine_m = st_own[...].astype(F32), sm_own[...]
    sib_s, sib_m = st_sib[...].astype(F32), sm_sib[...]
    lo_s, hi_s = jnp.where(low, mine_s, sib_s), jnp.where(low, sib_s, mine_s)
    lo_m, hi_m = jnp.where(low, mine_m, sib_m), jnp.where(low, sib_m, mine_m)
    s_half = width // 2

    def half_of(a, axis):
        parts = [lax.slice_in_dim(a, i * s_half, (i + 1) * s_half, axis=axis) for i in range(2)]
        return jnp.where(low, *parts)

    def half_column(row):
        return column_of(half_of(row, 1))

    def join(s_a, m_a, s_b, m_b):
        decay = m_b[0:1, :] * (m_a[2:3, 0:1] == m_b[1:2, 0:1]).astype(F32)
        return (
            s_a * half_column(decay) + s_b,
            small(m_a[0:1, :] * decay, m_a[1:2, 0:1], m_b[2:3, 0:1]),
        )

    chip_s, chip_m = join(half_of(lo_s, 0), lo_m, half_of(hi_s, 0), hi_m)
    st_cmp[...] = chip_s.astype(BF16)
    sm_cmp[...] = chip_m
    x = lax.rem(chip, 2)
    side = same_core(chip + 1 - 2 * x)
    cross_x = [
        remote(st_cmp, st_side, st_send.at[2], st_recv.at[2], side),
        remote(sm_cmp, sm_side, st_send.at[3], st_recv.at[3], side),
    ]
    for copy in cross_x:
        start(copy)
    for m in (2, 3):
        send_own(m)
    for copy in cross_x:
        copy.wait_recv()
    left = x == 0
    side_s, side_m = st_side[...].astype(F32), sm_side[...]
    plane_s, plane_m = join(
        jnp.where(left, chip_s, side_s), jnp.where(left, chip_m, side_m),
        jnp.where(left, side_s, chip_s), jnp.where(left, side_m, chip_m),
    )
    st_plane[...] = plane_s.astype(BF16)
    sm_plane[...] = plane_m

    def along_z(j):
        dev = same_core(lax.rem(chip + 2 * j, n_chip))
        n = 2 * j + 2
        return [
            remote(st_plane, st_in.at[j - 1], st_send.at[n], st_recv.at[n], dev),
            remote(sm_plane, sm_in.at[j - 1], st_send.at[n + 1], st_recv.at[n + 1], dev),
        ]

    for j in range(1, window + 1):

        @pl.when(chip + 2 * j < n_chip)
        def _():
            for copy in along_z(j):
                copy.start()

    relay((0, 1), 0)
    relay((2, 3), 0)
    for j in range(1, window + 1):

        @pl.when(chip >= 2 * j)
        def _():
            for copy in along_z(j):
                copy.wait_recv()

    entering = jnp.zeros((s_half, DV), F32)
    before = jnp.full((1, 1), -1.0, F32)
    for j in range(window, 0, -1):
        valid = chip >= 2 * j
        met = jnp.where(valid, sm_in[j - 1], 0.0)
        if j < window:
            linked = (before == met[1:2, 0:1]).astype(F32)
            entering = entering * half_column(met[0:1, :] * linked)
        entering = jnp.where(valid, entering + st_in[j - 1].astype(F32), 0.0)
        before = jnp.where(valid, met[2:3, 0:1], -1.0)
    linked = (before == side_m[1:2, 0:1]).astype(F32)
    through = entering * half_column(side_m[0:1, :] * linked) + side_s
    entering = jnp.where(left, entering, through)
    before = jnp.where(left, before, side_m[2:3, 0:1])
    s_at = pl.ds(pl.multiple_of(core * s_half, s_half), s_half)
    s_rest = pl.ds(pl.multiple_of((1 - core) * s_half, s_half), s_half)
    st_all[s_at, :] = entering.astype(BF16)
    n = 2 * window + 4
    start(remote(st_all.at[s_at, :], st_all.at[s_at, :], st_send.at[n], st_recv.at[n], sibling))
    remote(
        st_all.at[s_rest, :], st_all.at[s_rest, :], st_send.at[n], st_recv.at[n], sibling
    ).wait_recv()
    entering = st_all[...].astype(F32)
    linked = (before == sib_m[1:2, 0:1]).astype(F32)
    through = entering * column_of(sib_m[0:1, :] * linked) + sib_s
    before = jnp.where(low, before, sib_m[2:3, 0:1])
    state[...] = jnp.where(low, entering, through)

    for copy in loads[7:9]:
        copy.wait()

    def finish(b, carry):
        at = pl.ds(pl.multiple_of(b * SPAN, SPAN), SPAN)
        reach = (to_column(docs_ref[pl.ds(b, 1), :]) == before).astype(F32)
        qr = qrun[at, :]
        stacked = jnp.concatenate(
            [jnp.where(lane_head == h, qr, jnp.zeros_like(qr)) for h in range(heads)], axis=0
        )
        cross = dot1(stacked, state[...].astype(BF16))
        for h in range(heads):
            lanes = slice(h * DV, (h + 1) * DV)
            attn = local_out[at, lanes] + cross[h * SPAN : (h + 1) * SPAN] * reach
            scaled = (
                attn
                * lax.rsqrt(jnp.mean(attn * attn, axis=-1, keepdims=True) + eps)
                * head_gain_ref[...]
            )
            s = switch_ref[at, lanes].astype(F32)
            gated_all[group, at, lanes] = (scaled * (s / (1.0 + jnp.exp(-s)))).astype(BF16)
        return carry

    lax.fori_loop(0, n_block, finish, 0)
    g_to = remote(
        gated_all.at[group], gated_all.at[group], y_send.at[1], y_recv.at[1], across
    )
    start(g_to)

    p_back = remote(
        proj_all.at[1 - group, p_at, :], proj_all.at[1 - group, p_at, :],
        y_send.at[0], y_recv.at[0], across,
    )
    p_back.wait_recv()
    start(
        remote(
            proj_all.at[1 - group, p_at, :], proj_all.at[1 - group, p_at, :],
            y_send.at[2], y_recv.at[2], sibling,
        )
    )
    relay((0, 1), 1)
    for copy in loads[9:12]:
        copy.wait()
    p_rest = pl.ds(pl.multiple_of((1 - core) * p_half, p_half), p_half)
    remote(
        proj_all.at[1 - group, p_rest, :], proj_all.at[1 - group, p_rest, :],
        y_send.at[2], y_recv.at[2], sibling,
    ).wait_recv()
    remote(
        gated_all.at[1 - group], gated_all.at[1 - group], y_send.at[1], y_recv.at[1], across
    ).wait_recv()
    mix_rows = 256 if rows % 256 == 0 else rows
    mix_cols = 512 if model % 512 == 0 else model

    def mix(r, carry):
        at = pl.ds(pl.multiple_of(r * mix_rows, mix_rows), mix_rows)
        squares = jnp.zeros((mix_rows, 1), F32)
        for c in range(model // mix_cols):
            lanes = slice(c * mix_cols, (c + 1) * mix_cols)
            mixed = jnp.zeros((mix_rows, mix_cols), F32)
            for g in range(2):
                part = jnp.dot(
                    gated_all[g, at, :], proj_all[g, :, lanes], preferred_element_type=F32
                )
                mixed = mixed + part.astype(BF16).astype(F32)
            new = (first[at, lanes].astype(F32) + mixed).astype(BF16)
            first[at, lanes] = new
            wide = new.astype(F32)
            squares = squares + jnp.sum(wide * wide, axis=-1, keepdims=True)
        scale = lax.rsqrt(squares * (1.0 / model) + eps)
        for c in range(model // mix_cols):
            lanes = slice(c * mix_cols, (c + 1) * mix_cols)
            normed[at, lanes] = (
                first[at, lanes].astype(F32) * scale * gain_ref[:, lanes]
            ).astype(BF16)
        return carry

    lax.fori_loop(0, rows // mix_rows, mix, 0)

    relay((2, 3), 1)
    for i in range(2, reach - 1):
        relay((0, 1), i)
        relay((2, 3), i)
    loads[12].wait()
    swap_down(1 - core).wait_recv()
    for m in (4, 5):
        send_own(m)
    relay((0, 1), reach - 1)
    for m in (0, 1):
        loads[13 + m].wait()
    handed_part(0)
    def expand(t, carry):
        lanes = pl.ds(pl.multiple_of(t * TILE, TILE), TILE)
        g = jnp.dot(normed[...], gate_all[:, lanes], preferred_element_type=F32)
        u = jnp.dot(normed[...], up_all[:, lanes], preferred_element_type=F32)
        hidden[:, lanes] = (g / (1.0 + jnp.exp(-g)) * u).astype(BF16)
        return carry

    lax.fori_loop(0, split // TILE, expand, 0)

    relay((2, 3), reach - 1)
    relay((4,), 0)
    for m in (2, 3):
        loads[13 + m].wait()
    handed_part(2)
    lax.fori_loop(split // TILE, inner // TILE, expand, 0)

    own_rows = pl.ds(pl.multiple_of(group * half, half), half)

    def reduce_copy(m, lo, hi):
        lanes = pl.ds((m - 4) * unit_wide + lo * block, (hi - lo) * block)
        n = (m - 4) * (reach + 1) + (lo + 1) // 2
        return remote(
            normed.at[:half, lanes], recv_buf.at[:, lanes], red_send.at[0], red_recv.at[n], across
        )

    def shrink(m, lo, hi):
        lanes = slice((m - 4) * unit_wide + lo * block, (m - 4) * unit_wide + hi * block)
        a = jnp.dot(hidden[:half], down_all[:, lanes], preferred_element_type=F32)
        b = jnp.dot(hidden[half:], down_all[:, lanes], preferred_element_type=F32)
        normed[:half, lanes] = jnp.where(group == 0, b, a).astype(BF16)
        normed[half:, lanes] = jnp.where(group == 0, a, b).astype(BF16)
        reduce_copy(m, lo, hi).start()

    def shrink_last(m):
        lo, hi = n_chip - 1, n_chip
        lanes = slice((m - 4) * unit_wide + lo * block, (m - 4) * unit_wide + hi * block)
        part = half // 2
        for g, base in ((1 - group, 0), (group, half)):
            for i in range(2):
                at = pl.ds(pl.multiple_of(g * half + i * part, part), part)
                normed[base + i * part : base + (i + 1) * part, lanes] = jnp.dot(
                    hidden[at, :], down_all[:, lanes], preferred_element_type=F32
                ).astype(BF16)
            if base == 0:
                reduce_copy(m, lo, hi).start()

    def settle(m, lo, hi):
        reduce_copy(m, lo, hi).wait_recv()
        for slot in range(lo, hi):
            at = slice((m - 4) * unit_wide + slot * block, (m - 4) * unit_wide + (slot + 1) * block)
            lane = (near[slot] * 2 + m - 4) * block
            lanes = pl.ds(pl.multiple_of(lane, block), block)
            ffn = normed[half:, at].astype(F32) + recv_buf[:, at].astype(F32)
            out_ref[:, lanes] = (first[own_rows, lanes].astype(F32) + 0.5 * ffn).astype(BF16)

    shrink(4, 0, 1)
    shrink(5, 0, 1)
    relay((5,), 0)
    waiting = [(4, 0, 1), (5, 0, 1)]
    for i in range(1, reach):
        for m in (4, 5):
            if i > 1:
                relay((m,), i - 1)
            handed_down(m, i)
            shrink(m, 2 * i - 1, 2 * i + 1)
            settle(*waiting.pop(0))
            waiting.append((m, 2 * i - 1, 2 * i + 1))
    for m in (4, 5):
        relay((m,), reach - 1)
        handed_down(m, reach)
        shrink_last(m)
        waiting.append((m, n_chip - 1, n_chip))
        settle(*waiting.pop(0))
    for last in waiting:
        settle(*last)
    all_sent()
    remote(
        normed.at[:half, :], recv_buf, red_send.at[0], red_send.at[0], across
    ).wait_send()
    for copy in sent:
        copy.wait_send()
    for j in range(1, window + 1):

        @pl.when(chip + 2 * j < n_chip)
        def _():
            for copy in along_z(j):
                copy.wait_send()


def fused_per_device(
    skip_connection_stream,
    probing_vectors,
    addressing_vectors,
    mapped_payloads,
    emission_switch,
    lapse_preactivation,
    lapse_shift_entries,
    surplus_attenuation_terms,
    passage_label_per_token,
    attention_group_rescaler,
    emission_projector,
    perceptron_rescaler,
    switching_projector,
    widening_projector,
    shrinking_projector,
):
    rows, width = probing_vectors.shape
    group_w = mapped_payloads.shape[1]
    model = skip_connection_stream.shape[1]
    block, inner = switching_projector.shape
    n_sp, n_tp = lax.axis_size("sp"), lax.axis_size("tp")
    n_chip = n_sp // 2
    window = min(pl.cdiv(DOC_MOST, 4 * rows), n_chip // 2 - 1)
    tiles = inner // TILE
    split = TILE * pl.cdiv(tiles * 3, 5)
    half = rows // 2
    docs = passage_label_per_token.reshape(-1, 2 * SPAN)
    surplus = surplus_attenuation_terms.reshape(-1, 2 * SPAN)
    DMA = pltpu.SemaphoreType.DMA
    hbm = pl.BlockSpec(memory_space=pl.ANY)
    plan = (n_chip, window, split)
    return pl.pallas_call(
        functools.partial(fused_kernel, plan),
        out_shape=pltpu.VMEM((half, model), BF16),
        in_specs=[hbm] * 15,
        out_specs=vmem(1)[0],
        scratch_shapes=[
            pltpu.VMEM((1, width), F32),
            pltpu.VMEM((rows // (2 * SPAN), 2 * SPAN), jnp.int32),
            pltpu.VMEM((rows // (2 * SPAN), 2 * SPAN), F32),
            pltpu.VMEM((1, DV), F32),
            pltpu.VMEM((1, model), F32),
            pltpu.VMEM((rows // SPAN, SPAN), F32),
            pltpu.VMEM((rows // SPAN, SPAN), F32),
            pltpu.VMEM((model, inner), BF16),
            pltpu.VMEM((model, inner), BF16),
            pltpu.VMEM((inner, model), BF16),
            pltpu.VMEM((n_tp, group_w, model), BF16),
            pltpu.VMEM((n_tp, rows, group_w), BF16),
            pltpu.VMEM((rows, model), BF16),
            pltpu.VMEM((rows, model), BF16),
            pltpu.VMEM((rows, inner), BF16),
            pltpu.VMEM((rows, width), BF16),
            pltpu.VMEM((rows, width), BF16),
            pltpu.VMEM((rows, group_w), BF16),
            pltpu.VMEM((rows, group_w), BF16),
            pltpu.VMEM((rows, width), BF16),
            pltpu.VMEM((rows, group_w), F32),
            pltpu.VMEM((rows, width), BF16),
            pltpu.VMEM((width, DV), F32),
            pltpu.VMEM((8, width), F32),
            pltpu.VMEM((width, DV), BF16),
            pltpu.VMEM((8, width), F32),
            pltpu.VMEM((width, DV), BF16),
            pltpu.VMEM((8, width), F32),
            pltpu.VMEM((width // 2, DV), BF16),
            pltpu.VMEM((8, width), F32),
            pltpu.VMEM((width // 2, DV), BF16),
            pltpu.VMEM((8, width), F32),
            pltpu.VMEM((width // 2, DV), BF16),
            pltpu.VMEM((8, width), F32),
            pltpu.VMEM((window, width // 2, DV), BF16),
            pltpu.VMEM((window, 8, width), F32),
            pltpu.VMEM((width, DV), BF16),
            pltpu.VMEM((half, model), BF16),
            DMA((17,)),
            DMA((3,)),
            DMA((4, n_chip // 2)),
            DMA((4,)),
            DMA((4, n_chip // 2 + 1)),

            DMA((3,)),
            DMA((3,)),
            DMA((2 * window + 5,)),
            DMA((2 * window + 5,)),
            DMA((1,)),
            DMA((n_chip + 2,)),
        ],
        compiler_params=pltpu.CompilerParams(
            collective_id=0, has_side_effects=True, vmem_limit_bytes=62_000_000
        ),
        cost_estimate=pl.CostEstimate(
            flops=30_000_000_000, bytes_accessed=20_000_000, transcendentals=0
        ),
        name="fused_layer",
    )(
        skip_connection_stream,
        probing_vectors,
        addressing_vectors,
        mapped_payloads,
        emission_switch,
        lapse_preactivation,
        emission_projector,
        switching_projector,
        widening_projector,
        shrinking_projector,
        lapse_shift_entries[None, :],
        docs,
        surplus,
        attention_group_rescaler[None, :],
        perceptron_rescaler[None, :],
    )


def fits_fused(mesh, arrays):
    n_sp, n_tp = mesh.shape["sp"], mesh.shape["tp"]
    gate = arrays[12]
    block, inner = gate.shape[0] // n_sp, gate.shape[1] // n_tp
    even = n_sp % 8 == 0 and n_tp == 2
    return even and block % 128 == 0 and inner % TILE == 0 and 6 * gate.size // n_tp < 2**25 * 3 // 2


def solution(mesh):
    placed = (
        P("sp", None),
        P("sp", "tp"),
        P("sp", "tp"),
        P("sp", "tp"),
        P("sp", "tp"),
        P("sp", "tp"),
        P("tp"),
        P("sp"),
        P("sp"),
        P(),
        P("tp", None),
        P(),
        P("sp", "tp"),
        P("sp", "tp"),
        P("tp", "sp"),
    )

    def layer(*arrays):
        body = fused_per_device if fits_fused(mesh, arrays) else per_device
        return jax.shard_map(
            body, mesh=mesh, in_specs=placed, out_specs=P(("sp", "tp"), None), check_vma=False
        )(*arrays)

    return layer
```

```python
import functools

import jax
import jax.numpy as jnp
from jax import lax
from jax.experimental import pallas as pl
from jax.experimental.pallas import tpu as pltpu
from jax.sharding import PartitionSpec as P

DK = 64
DV = 128
BLOCK = 64
LIMIT = 80.0

eps = 1e-06
sharpness_factor = 16.0
HIGHEST = lax.Precision.HIGHEST
F32 = jnp.float32
BF16 = jnp.bfloat16


def dot0(a, b, precision=None):
    return lax.dot_general(
        a, b, (((0,), (0,)), ((), ())), precision=precision, preferred_element_type=F32
    )


def dot1(a, b, precision=None):
    return lax.dot_general(
        a, b, (((1,), (0,)), ((), ())), precision=precision, preferred_element_type=F32
    )


def local_pass(
    q_ref, k_ref, v_ref, lapse_ref, shift_ref, surplus_ref, doc_col_ref, doc_row_ref,
    out_ref, qrun_ref, state_ref, total_ref,
):
    length, width = q_ref.shape
    heads = width // DK
    span = BLOCK
    middle = span // 2
    rows = lax.broadcasted_iota(jnp.int32, (span, span), 0)
    cols = lax.broadcasted_iota(jnp.int32, (span, span), 1)
    lower = rows >= cols
    tril = lower.astype(F32)
    ones = jnp.ones((span, DV), F32)
    lane_head = lax.broadcasted_iota(jnp.int32, (span, width), 1) // DK
    head_mask = [(lane_head == h).astype(F32) for h in range(heads)]

    def per_head(a):
        return jnp.concatenate([(a * m).astype(BF16) for m in head_mask], axis=0)

    state = None
    offset = jnp.zeros((1, width), F32)
    for b in range(length // span):
        at = pl.ds(b * span, span)
        pre = lapse_ref[at, :].astype(F32) + shift_ref[...]
        ld = (jnp.minimum(pre, 0.0) - jnp.log1p(jnp.exp(-jnp.abs(pre)))) * (
            1.0 / sharpness_factor
        ) + surplus_ref[at, :]
        cum = dot1(tril, ld, HIGHEST)
        q = q_ref[at, :].astype(F32) * DK ** (-0.5)
        k = k_ref[at, :].astype(F32)
        v = v_ref[at, :]
        doc_col = doc_col_ref[at, :]
        doc_row = doc_row_ref[b : b + 1, :]
        tot = cum[span - 1 : span, :]
        centre = cum[middle : middle + 1, :]
        decayed = jnp.exp(cum)
        qd = q * decayed
        qrun_ref[at, :] = (qd * jnp.exp(offset)).astype(BF16)
        qs = q * jnp.exp(jnp.minimum(cum - centre, LIMIT))
        ks = (k * jnp.exp(jnp.minimum(centre - cum, LIMIT))).astype(BF16)
        scores = lax.dot_general(
            per_head(qs), ks, (((1,), (1,)), ((), ())), preferred_element_type=F32
        )
        same = (doc_col == doc_row) & lower
        if b > 0:
            last = doc_col_ref[b * span - 1 : b * span, :]
            valid = (doc_col == last).astype(F32)
            cross = dot1(per_head(qd), state.astype(BF16))
        for h in range(heads):
            piece = slice(h * span, (h + 1) * span)
            lanes = slice(h * DV, (h + 1) * DV)
            masked = jnp.where(same, scores[piece], 0.0).astype(BF16)
            res = dot1(masked, v[:, lanes])
            if b > 0:
                res = res + cross[piece] * valid
            out_ref[at, lanes] = res
        tail_doc = doc_col[span - 1 : span, :]
        tail_ok = (doc_col == tail_doc).astype(F32)
        kd = (k * jnp.exp(tot - cum) * tail_ok).astype(BF16)
        update = dot0(kd, v)
        update = jnp.concatenate(
            [update[h * DK : (h + 1) * DK, h * DV : (h + 1) * DV] for h in range(heads)], axis=0
        )
        if b > 0:
            keep = (tail_doc == last).astype(F32)
            state = state * (jnp.exp(dot0(ld, ones, HIGHEST)) * keep) + update
        else:
            state = update
        offset = offset + tot
    state_ref[...] = state
    total_ref[...] = offset


def finish_pass(out_ref, qrun_ref, entering_ref, reaches_ref, switch_ref, gain_ref, gated_ref):
    length, width = qrun_ref.shape
    heads = width // DK
    rows = 256 if length % 256 == 0 else length
    lane_head = lax.broadcasted_iota(jnp.int32, (rows, width), 1) // DK
    for r in range(length // rows):
        at = pl.ds(r * rows, rows)
        q = qrun_ref[at, :]
        reaches = reaches_ref[at, :]
        for h in range(heads):
            lanes = slice(h * DV, (h + 1) * DV)
            qh = jnp.where(lane_head == h, q, jnp.zeros_like(q))
            attn = out_ref[at, lanes] + dot1(qh, entering_ref[...]) * reaches
            normed = (
                attn
                * lax.rsqrt(jnp.mean(attn * attn, axis=-1, keepdims=True) + eps)
                * gain_ref[...]
            )
            s = switch_ref[at, lanes].astype(F32)
            gated_ref[at, lanes] = (normed * (s / (1.0 + jnp.exp(-s)))).astype(BF16)


def rms_rows(rows, gain):
    wide = rows.astype(F32)
    return (wide * lax.rsqrt(jnp.mean(wide * wide, axis=-1, keepdims=True) + eps) * gain).astype(
        BF16
    )


def ring_orders(n_sp):
    chips = n_sp // 2
    return list(range(0, chips, 2)) + list(range(1, chips, 2))[::-1]


def ring_pairs(n_sp, step):
    ring = ring_orders(n_sp)
    count = len(ring)
    return [
        (2 * ring[i] + core, 2 * ring[(i + step) % count] + core)
        for i in range(count)
        for core in (0, 1)
    ]


def swap_cores(a, n_sp):
    return lax.ppermute(a, "sp", [(i, i ^ 1) for i in range(n_sp)])


def ring_start(own, n_sp):
    return (
        lax.ppermute(own, "sp", ring_pairs(n_sp, 1)),
        lax.ppermute(own, "sp", ring_pairs(n_sp, -1)),
    )


def ring_rest(first, n_sp, axis):
    behind, ahead = [first[0]], [first[1]]
    count = n_sp // 2
    for _ in range((count - 1) // 2 - 1):
        behind.append(lax.ppermute(behind[-1], "sp", ring_pairs(n_sp, 1)))
        ahead.append(lax.ppermute(ahead[-1], "sp", ring_pairs(n_sp, -1)))
    size = first[0].shape[axis] // 2
    low = lax.slice_in_dim(behind[-1], 0, size, axis=axis)
    high = lax.slice_in_dim(ahead[-1], size, 2 * size, axis=axis)
    low = lax.ppermute(low, "sp", ring_pairs(n_sp, 1))
    high = lax.ppermute(high, "sp", ring_pairs(n_sp, -1))
    return behind, ahead, (low, high)


def vmem(n):
    return [pl.BlockSpec(memory_space=pltpu.VMEM)] * n


def per_device(
    skip_connection_stream,
    probing_vectors,
    addressing_vectors,
    mapped_payloads,
    emission_switch,
    lapse_preactivation,
    lapse_shift_entries,
    surplus_attenuation_terms,
    passage_label_per_token,
    attention_group_rescaler,
    emission_projector,
    perceptron_rescaler,
    switching_projector,
    widening_projector,
    shrinking_projector,
):
    rows_here, width = probing_vectors.shape
    heads = width // DK
    n_sp, n_tp = lax.axis_size("sp"), lax.axis_size("tp")
    place, group = lax.axis_index("sp"), lax.axis_index("tp")
    docs = passage_label_per_token

    def to_later(a, step):
        return lax.ppermute(a, "tp", [(i, (i + step) % n_tp) for i in range(n_tp)])

    both_w = jnp.concatenate([switching_projector, widening_projector], axis=1)
    both_first = ring_start(both_w, n_sp)
    down_first = ring_start(shrinking_projector, n_sp)
    projectors = [emission_projector] + [to_later(emission_projector, s) for s in range(1, n_tp)]

    local_out, qrun, state, total = pl.pallas_call(
        local_pass,
        out_shape=(
            jax.ShapeDtypeStruct((rows_here, heads * DV), F32),
            jax.ShapeDtypeStruct((rows_here, width), BF16),
            jax.ShapeDtypeStruct((width, DV), F32),
            jax.ShapeDtypeStruct((1, width), F32),
        ),
        in_specs=vmem(8),
        out_specs=tuple(vmem(4)),
        cost_estimate=pl.CostEstimate(
            flops=40_000_000_000, bytes_accessed=6_000_000, transcendentals=0
        ),
        name="local_pass",
    )(
        probing_vectors,
        addressing_vectors,
        mapped_payloads,
        lapse_preactivation,
        lapse_shift_entries[None, :],
        surplus_attenuation_terms[:, None],
        docs[:, None],
        docs.reshape(-1, BLOCK),
    )

    unbroken = (docs[0] == docs[-1]).astype(F32)
    ends = jnp.stack([docs[0], docs[-1]]).astype(BF16)
    small = jnp.concatenate([(jnp.exp(total[0]) * unbroken).astype(BF16), ends])
    tail_rows = 16 * pl.cdiv(small.size, 16 * DV)
    small = jnp.pad(small, (0, tail_rows * DV - small.size)).reshape(tail_rows, DV)
    packed = jnp.concatenate([state.astype(BF16), small], axis=0)
    half = (width + tail_rows) // 2
    first_half = lax.all_gather(packed[:half], "sp")
    packed, first_half = lax.optimization_barrier((packed, first_half))
    second_half = lax.all_gather(packed[half:], "sp")
    second_half, both_first = lax.optimization_barrier((second_half, both_first))
    packed = jnp.concatenate([first_half, second_half], axis=1)
    behind, ahead, opposite = ring_rest(both_first, n_sp, 1)
    down_first, opposite = lax.optimization_barrier((down_first, opposite))
    down_behind, down_ahead, down_opposite = ring_rest(down_first, n_sp, 0)

    ring = jnp.asarray(ring_orders(n_sp), jnp.int32)
    count = n_sp // 2
    spot = jnp.argmax(ring == place // 2)
    core = place % 2

    def chip_at(steps_behind):
        return ring[(spot - steps_behind + count) % count]

    chips = [chip_at(0)]
    chips += [chip_at(d + 1) for d in range(len(behind))]
    chips += [chip_at(-d - 1) for d in range(len(ahead))]
    chips += [chip_at(count // 2)]
    owners = [2 * c + core for c in chips] + [2 * c + 1 - core for c in chips]
    lows, highs = opposite
    here = [both_w] + behind + ahead + [jnp.concatenate([lows, highs], axis=1)]
    there = [swap_cores(a, n_sp) for a in [both_w] + behind + ahead]
    there += [jnp.concatenate([swap_cores(lows, n_sp), swap_cores(highs, n_sp)], axis=1)]
    hidden_width = switching_projector.shape[1]
    gate_w = jnp.concatenate([a[:, :hidden_width] for a in here + there], axis=0)
    up_w = jnp.concatenate([a[:, hidden_width:] for a in here + there], axis=0)
    down_here = [shrinking_projector] + down_behind + down_ahead
    down_there = [swap_cores(a, n_sp) for a in down_here]
    states = packed[:, :width]
    smalls = packed[:, width:].reshape(n_sp, -1).astype(F32)
    decays, first_doc, last_doc = smalls[:, :width], smalls[:, width], smalls[:, width + 1]
    before = jnp.concatenate([jnp.full((1,), -1.0, F32), last_doc[:-1]])
    decays = decays * (before == first_doc).astype(F32)[:, None]
    entering = jnp.zeros((width, DV), F32)
    for j in range(n_sp):
        entering = jnp.where(
            j < place, entering * decays[j][:, None] + states[j].astype(F32), entering
        )
    reaches = (docs.astype(F32) == before[place]).astype(F32)

    gated = pl.pallas_call(
        finish_pass,
        out_shape=jax.ShapeDtypeStruct((rows_here, heads * DV), BF16),
        in_specs=vmem(6),
        out_specs=vmem(1)[0],
        cost_estimate=pl.CostEstimate(
            flops=5_000_000_000, bytes_accessed=5_000_000, transcendentals=0
        ),
        name="finish_pass",
    )(
        local_out,
        qrun,
        entering.astype(BF16),
        reaches[:, None],
        emission_switch,
        attention_group_rescaler[None, :],
    )

    gateds = [gated] + [to_later(gated, s) for s in range(1, n_tp)]
    mixed = jnp.zeros((), F32)
    for rows, weight in zip(gateds, projectors):
        part = jnp.dot(rows, weight, preferred_element_type=F32).astype(BF16)
        mixed = mixed + part.astype(F32)
    first_all = (skip_connection_stream.astype(F32) + mixed).astype(BF16)
    normed = rms_rows(first_all, perceptron_rescaler)
    block = switching_projector.shape[0]

    def columns(a, owner):
        return lax.dynamic_slice_in_dim(a, owner * block, block, 1)

    ringed = jnp.concatenate([columns(normed, owner) for owner in owners], axis=1)
    gate = jnp.dot(ringed, gate_w, preferred_element_type=F32)
    upper = jnp.dot(ringed, up_w, preferred_element_type=F32)
    hidden = (jax.nn.silu(gate) * upper).astype(BF16)

    share = rows_here // n_tp

    def share_of(a, owner):
        return lax.dynamic_slice_in_dim(a, owner * share, share, 0)

    def reduced(weight):
        def down(owner):
            return jnp.dot(share_of(hidden, owner), weight, preferred_element_type=F32).astype(BF16)

        arrived = [to_later(down((group + s) % n_tp), s) for s in range(1, n_tp)]
        total = down(group).astype(F32)
        for part in arrived:
            total = total + part.astype(F32)
        return total

    late_here = jnp.concatenate(down_opposite, axis=0)
    late_there = jnp.concatenate([swap_cores(a, n_sp) for a in down_opposite], axis=0)
    near = (len(down_here) + 1) // 2
    order = [0] + [i + 1 + j * len(down_behind) for i in range(len(down_behind)) for j in (0, 1)]
    groups = [order[:near], order[near:], [len(down_here)]]
    down_here, down_there = down_here + [late_here], down_there + [late_there]
    first_own = share_of(first_all, group)
    out = first_own
    for members in groups:
        weight = jnp.concatenate(
            [down_here[i] for i in members] + [down_there[i] for i in members], axis=1
        )
        whose = [owners[i] for i in members] + [owners[len(chips) + i] for i in members]
        total = reduced(weight)
        for i, owner in enumerate(whose):
            start = (0, owner * block)
            piece = total[:, i * block : (i + 1) * block]
            base = lax.dynamic_slice(first_own, start, (share, block)).astype(F32)
            out = lax.dynamic_update_slice(out, (base + 0.5 * piece).astype(BF16), start)
    return out


MESH = pl.DeviceIdType.MESH
SPAN = BLOCK
TILE = 256
DOC_MOST = 6144


def local_copy(src, dst, sem):
    return pltpu.make_async_copy(src, dst, sem)


def column_of(row):
    first = lax.broadcasted_iota(jnp.int32, (8, row.shape[1]), 0) == 0
    return dot0(jnp.where(first, row, 0.0), jnp.ones((8, DV), F32), HIGHEST)


def ring_chip(spot, n_chip):
    return jnp.where(spot < n_chip // 2, 2 * spot, 2 * (n_chip - 1 - spot) + 1)


def ring_spot(chip, n_chip):
    return jnp.where(chip % 2 == 0, chip // 2, n_chip - 1 - chip // 2)


def fused_kernel(
    plan,
    skip_hbm, q_hbm, k_hbm, v_hbm, switch_hbm, lapse_hbm, proj_hbm, gate_hbm, up_hbm, down_hbm,
    shift_hbm, docs_hbm, surplus_hbm, head_gain_hbm, gain_hbm,
    out_ref,
    shift_ref, docs_in, surplus_in, head_gain_ref, gain_ref, docs_ref, surplus_ref,
    gate_all, up_all, down_all, proj_all, gated_all, first, normed, hidden,
    q_ref, k_ref, v_ref, switch_ref, lapse_ref, local_out, qrun, state, total,
    st_own, sm_own, st_sib, sm_sib, st_cmp, sm_cmp, st_side, sm_side, st_plane, sm_plane,
    st_in, sm_in, st_all,
    recv_buf,
    load_sem, ici_send, ici_recv, d2d_send, d2d_recv,
    y_send, y_recv, st_send, st_recv, red_send, red_recv,
):
    n_chip, window, split = plan
    rows, width = q_ref.shape
    heads = width // DK
    group_w = heads * DV
    model = normed.shape[1]
    inner = hidden.shape[1]
    block = gate_hbm.shape[0]
    half = rows // 2

    place = lax.axis_index("sp")
    group = lax.axis_index("tp")
    core = lax.rem(place, 2)
    chip = place // 2
    reach = n_chip // 2
    spot = ring_spot(chip, n_chip)
    steps = [0] + [d for i in range(1, reach) for d in (i, -i)] + [reach]
    near = [ring_chip(lax.rem(spot + d + n_chip, n_chip), n_chip) for d in steps]
    sibling = {"sp": chip * 2 + 1 - core}
    across = {"tp": 1 - group}

    def same_core(c):
        return {"sp": c * 2 + core}

    ahead, behind = same_core(near[1]), same_core(near[2])

    def slot_of(d):
        return steps.index(d if -reach < d else d + n_chip)

    barrier = pltpu.get_barrier_semaphore()
    for j in range(1, n_chip):
        pl.semaphore_signal(
            barrier, inc=1, device_id=same_core(lax.rem(chip + j, n_chip)), device_id_type=MESH
        )
    pl.semaphore_signal(barrier, inc=1, device_id=sibling, device_id_type=MESH)
    pl.semaphore_signal(barrier, inc=1, device_id=across, device_id_type=MESH)
    pl.semaphore_wait(barrier, n_chip + 1)

    sent = []

    def remote(src, dst, send, recv, dev):
        return pltpu.make_async_remote_copy(
            src_ref=src, dst_ref=dst, send_sem=send, recv_sem=recv, device_id=dev,
            device_id_type=MESH,
        )

    def start(copy):
        copy.start()
        sent.append(copy)

    cols = [(0, split), (split, inner - split)]
    k_half = inner // 2
    unit_rows = [block] * 4 + [k_half] * 2
    unit_wide = n_chip * block

    def own_view(m, r0, nr):
        c0, nc = cols[m // 2]
        return (gate_hbm, up_hbm)[m % 2].at[pl.ds(r0, nr), pl.ds(c0, nc)]

    def down_lanes(m, slot):
        return pl.ds((m - 4) * unit_wide + slot * block, block)

    def view(m, slot, there, who, r0, nr):
        if m < 4:
            c0, nc = cols[m // 2]
            row = pl.multiple_of((near[slot] * 2 + who) * block + r0, 16)
            return (gate_all, up_all)[m % 2].at[pl.ds(row, nr), pl.ds(c0, nc)]
        row = pl.multiple_of(who * k_half + r0, 16)
        return down_all.at[pl.ds(row, nr), down_lanes(m, slot_of(steps[slot] - there))]

    def piece(m, i, forward):
        nr = unit_rows[m]
        if i < reach - 1:
            return 0, nr
        return (0, nr // 2) if forward else (nr // 2, nr - nr // 2)

    def joint(m):
        return m // 2 if m < 4 else m - 2

    def kind(m):
        return m % 2 if m < 4 else 2

    def hop(m, i, forward):
        r0, nr = piece(m, i, forward)
        sign = 1 if forward else -1
        slot = slot_of(-sign * i)
        src = own_view(m, r0, nr) if i == 0 and m < 4 else view(m, slot, 0, core, r0, nr)
        remote(
            src, view(m, slot, sign, core, r0, nr), ici_send.at[kind(m)], ici_recv.at[joint(m), i],
            ahead if forward else behind,
        ).start()

    def bytes_of(m, units):
        if m < 4:
            c0, nc = cols[m // 2]
            return gate_all.at[pl.ds(0, units * block), pl.ds(c0, nc)]
        return down_all.at[pl.ds(0, k_half), pl.ds(0, units * block)]

    def await_bytes(at, sem):
        remote(at, at, sem, sem, ahead).wait_recv()

    def landed(m, i):
        n = (2 if m < 4 else 1) * (2 if i + 1 < reach else 1)
        await_bytes(bytes_of(m, n), ici_recv.at[joint(m), i])

    def hand(m, slot):
        nr = unit_rows[m]
        at = view(m, slot, 0, core, 0, nr)
        src = own_view(m, 0, nr) if slot == 0 else at
        step = (slot + 1) // 2 if m >= 4 else 0
        remote(
            src, at, d2d_send.at[kind(m)], d2d_recv.at[joint(m), step], sibling
        ).start()

    def handed_part(m):
        await_bytes(bytes_of(m, 2 * n_chip), d2d_recv.at[joint(m), 0])

    def handed_down(m, i):
        n = 2 if i < reach else 1
        await_bytes(bytes_of(m, n), d2d_recv.at[joint(m), i])

    def all_sent():
        for n in range(2):
            at = (gate_all, up_all)[n].at[pl.ds(0, (n_chip - 1) * block), :]
            remote(at, at, ici_send.at[n], ici_send.at[n], ahead).wait_send()
            at = (gate_all, up_all)[n].at[pl.ds(0, n_chip * block), :]
            remote(at, at, d2d_send.at[n], d2d_send.at[n], sibling).wait_send()
        at = down_all.at[:, pl.ds(0, (n_chip - 1) * block)]
        remote(at, at, ici_send.at[2], ici_send.at[2], ahead).wait_send()
        remote(at, at, d2d_send.at[2], d2d_send.at[2], sibling).wait_send()

    def own_lanes(who):
        lane = pl.multiple_of(who * unit_wide, block)
        return down_all.at[:, pl.ds(lane, block)]

    def swap_down(who):
        at = own_lanes(who)
        src = down_hbm if who is core else at
        return remote(src, at, d2d_send.at[3], d2d_recv.at[2, 0], sibling)

    def send_own(m):
        hop(m, 0, True)
        hop(m, 0, False)

    def relay(units, i):
        landed(units[0], i)
        for m in units:
            if i + 1 < reach:
                hop(m, i + 1, True)
                hop(m, i + 1, False)
        for m in units:
            if i + 1 < reach:
                hand(m, slot_of(i + 1))
                hand(m, slot_of(-i - 1))
            else:
                hand(m, slot_of(reach))

    for m in range(2):
        send_own(m)
    p_half = proj_hbm.shape[0] // 2
    p_at = pl.ds(pl.multiple_of(core * p_half, p_half), p_half)
    p_to = remote(
        proj_hbm.at[p_at, :], proj_all.at[group, p_at, :], y_send.at[0], y_recv.at[0], across
    )
    start(p_to)
    pairs = [
        (q_hbm, q_ref), (k_hbm, k_ref), (v_hbm, v_ref), (lapse_hbm, lapse_ref),
        (shift_hbm, shift_ref), (docs_hbm, docs_in), (surplus_hbm, surplus_in),
        (switch_hbm, switch_ref), (head_gain_hbm, head_gain_ref),
        (skip_hbm, first), (gain_hbm, gain_ref), (proj_hbm, proj_all.at[group]),
        (down_hbm, own_lanes(core)),
    ] + [(own_view(m, 0, block), view(m, 0, 0, core, 0, block)) for m in range(4)]
    loads = [local_copy(src, dst, load_sem.at[i]) for i, (src, dst) in enumerate(pairs)]
    for copy in loads:
        copy.start()
    for m in range(4):
        hand(m, 0)
    start(swap_down(core))
    for copy in loads[:7]:
        copy.wait()
    for i in range(rows // (2 * SPAN)):
        for j in range(2):
            at = slice(2 * i + j, 2 * i + j + 1)
            lanes = slice(j * SPAN, (j + 1) * SPAN)
            docs_ref[at, :] = docs_in[i : i + 1, lanes].astype(F32)
            surplus_ref[at, :] = surplus_in[i : i + 1, lanes]

    middle = SPAN // 2
    r_i = lax.broadcasted_iota(jnp.int32, (SPAN, SPAN), 0)
    c_i = lax.broadcasted_iota(jnp.int32, (SPAN, SPAN), 1)
    lane_head = lax.broadcasted_iota(jnp.int32, (SPAN, width), 1) // DK
    head_mask = [(lane_head == h).astype(F32) for h in range(heads)]

    def per_head(a):
        return jnp.concatenate([(a * m).astype(BF16) for m in head_mask], axis=0)

    def to_column(row):
        return jnp.sum(jnp.where(r_i == c_i, row, 0.0), axis=1, keepdims=True)

    state[...] = jnp.zeros_like(state)
    total[...] = jnp.zeros_like(total)
    n_block = rows // SPAN

    def attend(b, last):
        lower = r_i >= c_i
        at = pl.ds(pl.multiple_of(b * SPAN, SPAN), SPAN)
        doc_row = docs_ref[pl.ds(b, 1), :]
        doc_col = to_column(doc_row)
        sur_col = to_column(surplus_ref[pl.ds(b, 1), :])
        pre = lapse_ref[at, :].astype(F32) + shift_ref[...]
        ld = (jnp.minimum(pre, 0.0) - jnp.log1p(jnp.exp(-jnp.abs(pre)))) * (
            1.0 / sharpness_factor
        ) + sur_col
        cum = dot1(lower.astype(F32), ld, HIGHEST)
        qb = q_ref[at, :].astype(F32) * DK ** (-0.5)
        kb = k_ref[at, :].astype(F32)
        vb = v_ref[at, :]
        tot = cum[SPAN - 1 : SPAN, :]
        centre = cum[middle : middle + 1, :]
        qd = qb * jnp.exp(cum)
        offset = total[0:1, :]
        qrun[at, :] = (qd * jnp.exp(offset)).astype(BF16)
        qs = qb * jnp.exp(jnp.minimum(cum - centre, LIMIT))
        ks = (kb * jnp.exp(jnp.minimum(centre - cum, LIMIT))).astype(BF16)
        scores = lax.dot_general(
            per_head(qs), ks, (((1,), (1,)), ((), ())), preferred_element_type=F32
        )
        same = (doc_col == doc_row) & lower
        valid = (doc_col == last).astype(F32)
        cross = dot1(per_head(qd), state[...].astype(BF16))
        for h in range(heads):
            piece = slice(h * SPAN, (h + 1) * SPAN)
            lanes = slice(h * DV, (h + 1) * DV)
            masked = jnp.where(same, scores[piece], 0.0).astype(BF16)
            local_out[at, lanes] = dot1(masked, vb[:, lanes]) + cross[piece] * valid
        tail_doc = doc_row[:, SPAN - 1 : SPAN]
        tail_ok = (doc_col == tail_doc).astype(F32)
        kd = (kb * jnp.exp(tot - cum) * tail_ok).astype(BF16)
        update = dot0(kd, vb)
        update = jnp.concatenate(
            [update[h * DK : (h + 1) * DK, h * DV : (h + 1) * DV] for h in range(heads)], axis=0
        )
        keep = (tail_doc == last).astype(F32)
        state[...] = state[...] * (column_of(jnp.exp(tot)) * keep) + update
        total[...] = total[...] + tot
        return tail_doc

    last_own = lax.fori_loop(0, n_block, attend, jnp.full((1, 1), -1.0, F32))

    first_own = docs_ref[0:1, 0:1]
    row8 = lax.broadcasted_iota(jnp.int32, (8, width), 0)

    def small(decay, first_doc, last_doc):
        return jnp.where(row8 == 0, decay, jnp.where(row8 == 1, first_doc, last_doc))

    unbroken = (first_own == last_own).astype(F32)
    st_own[...] = state[...].astype(BF16)
    sm_own[...] = small(jnp.exp(total[0:1, :]) * unbroken, first_own, last_own)

    swap = [
        remote(st_own, st_sib, st_send.at[0], st_recv.at[0], sibling),
        remote(sm_own, sm_sib, st_send.at[1], st_recv.at[1], sibling),
    ]
    for copy in swap:
        start(copy)
    for copy in swap:
        copy.wait_recv()
    low = core == 0
    mine_s, mine_m = st_own[...].astype(F32), sm_own[...]
    sib_s, sib_m = st_sib[...].astype(F32), sm_sib[...]
    lo_s, hi_s = jnp.where(low, mine_s, sib_s), jnp.where(low, sib_s, mine_s)
    lo_m, hi_m = jnp.where(low, mine_m, sib_m), jnp.where(low, sib_m, mine_m)
    s_half = width // 2

    def half_of(a, axis):
        parts = [lax.slice_in_dim(a, i * s_half, (i + 1) * s_half, axis=axis) for i in range(2)]
        return jnp.where(low, *parts)

    def half_column(row):
        return column_of(half_of(row, 1))

    def join(s_a, m_a, s_b, m_b):
        decay = m_b[0:1, :] * (m_a[2:3, 0:1] == m_b[1:2, 0:1]).astype(F32)
        return (
            s_a * half_column(decay) + s_b,
            small(m_a[0:1, :] * decay, m_a[1:2, 0:1], m_b[2:3, 0:1]),
        )

    chip_s, chip_m = join(half_of(lo_s, 0), lo_m, half_of(hi_s, 0), hi_m)
    st_cmp[...] = chip_s.astype(BF16)
    sm_cmp[...] = chip_m
    x = lax.rem(chip, 2)
    side = same_core(chip + 1 - 2 * x)
    cross_x = [
        remote(st_cmp, st_side, st_send.at[2], st_recv.at[2], side),
        remote(sm_cmp, sm_side, st_send.at[3], st_recv.at[3], side),
    ]
    for copy in cross_x:
        start(copy)
    for m in (2, 3):
        send_own(m)
    for copy in cross_x:
        copy.wait_recv()
    left = x == 0
    side_s, side_m = st_side[...].astype(F32), sm_side[...]
    plane_s, plane_m = join(
        jnp.where(left, chip_s, side_s), jnp.where(left, chip_m, side_m),
        jnp.where(left, side_s, chip_s), jnp.where(left, side_m, chip_m),
    )
    st_plane[...] = plane_s.astype(BF16)
    sm_plane[...] = plane_m

    def along_z(j):
        dev = same_core(lax.rem(chip + 2 * j, n_chip))
        n = 2 * j + 2
        return [
            remote(st_plane, st_in.at[j - 1], st_send.at[n], st_recv.at[n], dev),
            remote(sm_plane, sm_in.at[j - 1], st_send.at[n + 1], st_recv.at[n + 1], dev),
        ]

    for j in range(1, window + 1):

        @pl.when(chip + 2 * j < n_chip)
        def _():
            for copy in along_z(j):
                copy.start()

    relay((0, 1), 0)
    relay((2, 3), 0)
    for j in range(1, window + 1):

        @pl.when(chip >= 2 * j)
        def _():
            for copy in along_z(j):
                copy.wait_recv()

    entering = jnp.zeros((s_half, DV), F32)
    before = jnp.full((1, 1), -1.0, F32)
    for j in range(window, 0, -1):
        valid = chip >= 2 * j
        met = jnp.where(valid, sm_in[j - 1], 0.0)
        if j < window:
            linked = (before == met[1:2, 0:1]).astype(F32)
            entering = entering * half_column(met[0:1, :] * linked)
        entering = jnp.where(valid, entering + st_in[j - 1].astype(F32), 0.0)
        before = jnp.where(valid, met[2:3, 0:1], -1.0)
    linked = (before == side_m[1:2, 0:1]).astype(F32)
    through = entering * half_column(side_m[0:1, :] * linked) + side_s
    entering = jnp.where(left, entering, through)
    before = jnp.where(left, before, side_m[2:3, 0:1])
    s_at = pl.ds(pl.multiple_of(core * s_half, s_half), s_half)
    s_rest = pl.ds(pl.multiple_of((1 - core) * s_half, s_half), s_half)
    st_all[s_at, :] = entering.astype(BF16)
    n = 2 * window + 4
    start(remote(st_all.at[s_at, :], st_all.at[s_at, :], st_send.at[n], st_recv.at[n], sibling))
    remote(
        st_all.at[s_rest, :], st_all.at[s_rest, :], st_send.at[n], st_recv.at[n], sibling
    ).wait_recv()
    entering = st_all[...].astype(F32)
    linked = (before == sib_m[1:2, 0:1]).astype(F32)
    through = entering * column_of(sib_m[0:1, :] * linked) + sib_s
    before = jnp.where(low, before, sib_m[2:3, 0:1])
    state[...] = jnp.where(low, entering, through)

    for copy in loads[7:9]:
        copy.wait()

    def finish(b, carry):
        at = pl.ds(pl.multiple_of(b * SPAN, SPAN), SPAN)
        reach = (to_column(docs_ref[pl.ds(b, 1), :]) == before).astype(F32)
        qr = qrun[at, :]
        stacked = jnp.concatenate(
            [jnp.where(lane_head == h, qr, jnp.zeros_like(qr)) for h in range(heads)], axis=0
        )
        cross = dot1(stacked, state[...].astype(BF16))
        for h in range(heads):
            lanes = slice(h * DV, (h + 1) * DV)
            attn = local_out[at, lanes] + cross[h * SPAN : (h + 1) * SPAN] * reach
            scaled = (
                attn
                * lax.rsqrt(jnp.mean(attn * attn, axis=-1, keepdims=True) + eps)
                * head_gain_ref[...]
            )
            s = switch_ref[at, lanes].astype(F32)
            gated_all[group, at, lanes] = (scaled * (s / (1.0 + jnp.exp(-s)))).astype(BF16)
        return carry

    lax.fori_loop(0, n_block, finish, 0)
    g_to = remote(
        gated_all.at[group], gated_all.at[group], y_send.at[1], y_recv.at[1], across
    )
    start(g_to)

    p_back = remote(
        proj_all.at[1 - group, p_at, :], proj_all.at[1 - group, p_at, :],
        y_send.at[0], y_recv.at[0], across,
    )
    p_back.wait_recv()
    start(
        remote(
            proj_all.at[1 - group, p_at, :], proj_all.at[1 - group, p_at, :],
            y_send.at[2], y_recv.at[2], sibling,
        )
    )
    relay((0, 1), 1)
    for copy in loads[9:12]:
        copy.wait()
    p_rest = pl.ds(pl.multiple_of((1 - core) * p_half, p_half), p_half)
    remote(
        proj_all.at[1 - group, p_rest, :], proj_all.at[1 - group, p_rest, :],
        y_send.at[2], y_recv.at[2], sibling,
    ).wait_recv()
    remote(
        gated_all.at[1 - group], gated_all.at[1 - group], y_send.at[1], y_recv.at[1], across
    ).wait_recv()
    mix_rows = 256 if rows % 256 == 0 else rows
    mix_cols = 512 if model % 512 == 0 else model

    def mix(r, carry):
        at = pl.ds(pl.multiple_of(r * mix_rows, mix_rows), mix_rows)
        squares = jnp.zeros((mix_rows, 1), F32)
        for c in range(model // mix_cols):
            lanes = slice(c * mix_cols, (c + 1) * mix_cols)
            mixed = jnp.zeros((mix_rows, mix_cols), F32)
            for g in range(2):
                part = jnp.dot(
                    gated_all[g, at, :], proj_all[g, :, lanes], preferred_element_type=F32
                )
                mixed = mixed + part.astype(BF16).astype(F32)
            new = (first[at, lanes].astype(F32) + mixed).astype(BF16)
            first[at, lanes] = new
            wide = new.astype(F32)
            squares = squares + jnp.sum(wide * wide, axis=-1, keepdims=True)
        scale = lax.rsqrt(squares * (1.0 / model) + eps)
        for c in range(model // mix_cols):
            lanes = slice(c * mix_cols, (c + 1) * mix_cols)
            normed[at, lanes] = (
                first[at, lanes].astype(F32) * scale * gain_ref[:, lanes]
            ).astype(BF16)
        return carry

    lax.fori_loop(0, rows // mix_rows, mix, 0)

    relay((2, 3), 1)
    for i in range(2, reach - 1):
        relay((0, 1), i)
        relay((2, 3), i)
    loads[12].wait()
    swap_down(1 - core).wait_recv()
    for m in (4, 5):
        send_own(m)
    relay((0, 1), reach - 1)
    for m in (0, 1):
        loads[13 + m].wait()
    handed_part(0)
    def expand(t, carry):
        lanes = pl.ds(pl.multiple_of(t * TILE, TILE), TILE)
        g = jnp.dot(normed[...], gate_all[:, lanes], preferred_element_type=F32)
        u = jnp.dot(normed[...], up_all[:, lanes], preferred_element_type=F32)
        hidden[:, lanes] = (g / (1.0 + jnp.exp(-g)) * u).astype(BF16)
        return carry

    lax.fori_loop(0, split // TILE, expand, 0)

    relay((2, 3), reach - 1)
    relay((4,), 0)
    for m in (2, 3):
        loads[13 + m].wait()
    handed_part(2)
    lax.fori_loop(split // TILE, inner // TILE, expand, 0)

    own_rows = pl.ds(pl.multiple_of(group * half, half), half)

    def reduce_copy(m, lo, hi):
        lanes = pl.ds((m - 4) * unit_wide + lo * block, (hi - lo) * block)
        n = (m - 4) * (reach + 1) + (lo + 1) // 2
        return remote(
            normed.at[:half, lanes], recv_buf.at[:, lanes], red_send.at[0], red_recv.at[n], across
        )

    def shrink(m, lo, hi):
        lanes = slice((m - 4) * unit_wide + lo * block, (m - 4) * unit_wide + hi * block)
        a = jnp.dot(hidden[:half], down_all[:, lanes], preferred_element_type=F32)
        b = jnp.dot(hidden[half:], down_all[:, lanes], preferred_element_type=F32)
        normed[:half, lanes] = jnp.where(group == 0, b, a).astype(BF16)
        normed[half:, lanes] = jnp.where(group == 0, a, b).astype(BF16)
        reduce_copy(m, lo, hi).start()

    def shrink_last(m):
        lo, hi = n_chip - 1, n_chip
        base = (m - 4) * unit_wide + lo * block
        lanes = slice(base, base + block)
        part = half // 2
        mine = pl.ds(pl.multiple_of(core * k_half, block), k_half)
        theirs = pl.ds(pl.multiple_of((1 - core) * k_half, block), k_half)
        spans = [
            pl.ds(pl.multiple_of(g * half + i * part, part), part)
            for g in (1 - group, group)
            for i in range(2)
        ]
        sums = [
            jnp.dot(hidden[at, mine], down_all[mine, lanes], preferred_element_type=F32)
            for at in spans
        ]
        handed_down(m, reach)
        n = (m - 4) * (reach + 1) + (lo + 1) // 2
        for i, at in enumerate(spans):
            more = jnp.dot(hidden[at, theirs], down_all[theirs, lanes], preferred_element_type=F32)
            put = slice(i * part, (i + 1) * part)
            normed[put, lanes] = (sums[i] + more).astype(BF16)
            if i < 2:
                remote(
                    normed.at[put, lanes], recv_buf.at[put, lanes],
                    red_send.at[0], red_recv.at[n], across,
                ).start()

    def settle(m, lo, hi):
        reduce_copy(m, lo, hi).wait_recv()
        for slot in range(lo, hi):
            at = slice((m - 4) * unit_wide + slot * block, (m - 4) * unit_wide + (slot + 1) * block)
            lane = (near[slot] * 2 + m - 4) * block
            lanes = pl.ds(pl.multiple_of(lane, block), block)
            ffn = normed[half:, at].astype(F32) + recv_buf[:, at].astype(F32)
            out_ref[:, lanes] = (first[own_rows, lanes].astype(F32) + 0.5 * ffn).astype(BF16)

    shrink(4, 0, 1)
    shrink(5, 0, 1)
    relay((5,), 0)
    waiting = [(4, 0, 1), (5, 0, 1)]
    for i in range(1, reach):
        for m in (4, 5):
            if i > 1:
                relay((m,), i - 1)
            handed_down(m, i)
            shrink(m, 2 * i - 1, 2 * i + 1)
            settle(*waiting.pop(0))
            waiting.append((m, 2 * i - 1, 2 * i + 1))
    for m in (4, 5):
        relay((m,), reach - 1)
        shrink_last(m)
        waiting.append((m, n_chip - 1, n_chip))
        settle(*waiting.pop(0))
    for last in waiting:
        settle(*last)
    all_sent()
    remote(
        normed.at[:half, :], recv_buf, red_send.at[0], red_send.at[0], across
    ).wait_send()
    for copy in sent:
        copy.wait_send()
    for j in range(1, window + 1):

        @pl.when(chip + 2 * j < n_chip)
        def _():
            for copy in along_z(j):
                copy.wait_send()


def fused_per_device(
    skip_connection_stream,
    probing_vectors,
    addressing_vectors,
    mapped_payloads,
    emission_switch,
    lapse_preactivation,
    lapse_shift_entries,
    surplus_attenuation_terms,
    passage_label_per_token,
    attention_group_rescaler,
    emission_projector,
    perceptron_rescaler,
    switching_projector,
    widening_projector,
    shrinking_projector,
):
    rows, width = probing_vectors.shape
    group_w = mapped_payloads.shape[1]
    model = skip_connection_stream.shape[1]
    block, inner = switching_projector.shape
    n_sp, n_tp = lax.axis_size("sp"), lax.axis_size("tp")
    n_chip = n_sp // 2
    window = min(pl.cdiv(DOC_MOST, 4 * rows), n_chip // 2 - 1)
    tiles = inner // TILE
    split = TILE * pl.cdiv(tiles * 3, 5)
    half = rows // 2
    docs = passage_label_per_token.reshape(-1, 2 * SPAN)
    surplus = surplus_attenuation_terms.reshape(-1, 2 * SPAN)
    DMA = pltpu.SemaphoreType.DMA
    hbm = pl.BlockSpec(memory_space=pl.ANY)
    plan = (n_chip, window, split)
    return pl.pallas_call(
        functools.partial(fused_kernel, plan),
        out_shape=pltpu.VMEM((half, model), BF16),
        in_specs=[hbm] * 15,
        out_specs=vmem(1)[0],
        scratch_shapes=[
            pltpu.VMEM((1, width), F32),
            pltpu.VMEM((rows // (2 * SPAN), 2 * SPAN), jnp.int32),
            pltpu.VMEM((rows // (2 * SPAN), 2 * SPAN), F32),
            pltpu.VMEM((1, DV), F32),
            pltpu.VMEM((1, model), F32),
            pltpu.VMEM((rows // SPAN, SPAN), F32),
            pltpu.VMEM((rows // SPAN, SPAN), F32),
            pltpu.VMEM((model, inner), BF16),
            pltpu.VMEM((model, inner), BF16),
            pltpu.VMEM((inner, model), BF16),
            pltpu.VMEM((n_tp, group_w, model), BF16),
            pltpu.VMEM((n_tp, rows, group_w), BF16),
            pltpu.VMEM((rows, model), BF16),
            pltpu.VMEM((rows, model), BF16),
            pltpu.VMEM((rows, inner), BF16),
            pltpu.VMEM((rows, width), BF16),
            pltpu.VMEM((rows, width), BF16),
            pltpu.VMEM((rows, group_w), BF16),
            pltpu.VMEM((rows, group_w), BF16),
            pltpu.VMEM((rows, width), BF16),
            pltpu.VMEM((rows, group_w), F32),
            pltpu.VMEM((rows, width), BF16),
            pltpu.VMEM((width, DV), F32),
            pltpu.VMEM((8, width), F32),
            pltpu.VMEM((width, DV), BF16),
            pltpu.VMEM((8, width), F32),
            pltpu.VMEM((width, DV), BF16),
            pltpu.VMEM((8, width), F32),
            pltpu.VMEM((width // 2, DV), BF16),
            pltpu.VMEM((8, width), F32),
            pltpu.VMEM((width // 2, DV), BF16),
            pltpu.VMEM((8, width), F32),
            pltpu.VMEM((width // 2, DV), BF16),
            pltpu.VMEM((8, width), F32),
            pltpu.VMEM((window, width // 2, DV), BF16),
            pltpu.VMEM((window, 8, width), F32),
            pltpu.VMEM((width, DV), BF16),
            pltpu.VMEM((half, model), BF16),
            DMA((17,)),
            DMA((3,)),
            DMA((4, n_chip // 2)),
            DMA((4,)),
            DMA((4, n_chip // 2 + 1)),

            DMA((3,)),
            DMA((3,)),
            DMA((2 * window + 5,)),
            DMA((2 * window + 5,)),
            DMA((1,)),
            DMA((n_chip + 2,)),
        ],
        compiler_params=pltpu.CompilerParams(
            collective_id=0, has_side_effects=True, vmem_limit_bytes=63_500_000
        ),
        cost_estimate=pl.CostEstimate(
            flops=30_000_000_000, bytes_accessed=20_000_000, transcendentals=0
        ),
        name="fused_layer",
    )(
        skip_connection_stream,
        probing_vectors,
        addressing_vectors,
        mapped_payloads,
        emission_switch,
        lapse_preactivation,
        emission_projector,
        switching_projector,
        widening_projector,
        shrinking_projector,
        lapse_shift_entries[None, :],
        docs,
        surplus,
        attention_group_rescaler[None, :],
        perceptron_rescaler[None, :],
    )


def fits_fused(mesh, arrays):
    n_sp, n_tp = mesh.shape["sp"], mesh.shape["tp"]
    gate = arrays[12]
    block, inner = gate.shape[0] // n_sp, gate.shape[1] // n_tp
    even = n_sp % 8 == 0 and n_tp == 2
    return even and block % 128 == 0 and inner % TILE == 0 and 6 * gate.size // n_tp < 2**25 * 3 // 2


def solution(mesh):
    placed = (
        P("sp", None),
        P("sp", "tp"),
        P("sp", "tp"),
        P("sp", "tp"),
        P("sp", "tp"),
        P("sp", "tp"),
        P("tp"),
        P("sp"),
        P("sp"),
        P(),
        P("tp", None),
        P(),
        P("sp", "tp"),
        P("sp", "tp"),
        P("tp", "sp"),
    )

    def layer(*arrays):
        body = fused_per_device if fits_fused(mesh, arrays) else per_device
        return jax.shard_map(
            body, mesh=mesh, in_specs=placed, out_specs=P(("sp", "tp"), None), check_vma=False
        )(*arrays)

    return layer
```
